256 devices in a mesh: fs: 32 (over z, y), tp: 8 (over x, core).
Axes of the slice: x: 4, y: 4, z: 8, core: 2. Of those that a mesh axis runs over, the one named last changes fastest.
Arguments:
- tokens: bfloat16 [12288, 2048], P(('fs', 'tp')), may hold values from -6 to 6
- ffn1_gain: float32 [2048], replicated, may hold values from 0.1 to 1.9
- ffn1_gate: bfloat16 [2048, 5632], P('fs', 'tp'), may hold values from -0.125 to 0.125
- ffn1_up: bfloat16 [2048, 5632], P('fs', 'tp'), may hold values from -0.125 to 0.125
- ffn1_down: bfloat16 [5632, 2048], P('tp', 'fs'), may hold values from -0.078125 to 0.078125
- mix_gain: float32 [2048], replicated, may hold values from 0.1 to 1.9
- lru_in_weight: bfloat16 [2048, 1536], P('fs', 'tp'), may hold values from -0.125 to 0.125
- lru_gate_weight: bfloat16 [2048, 1536], P('fs', 'tp'), may hold values from -0.125 to 0.125
- conv_weight: bfloat16 [4, 1536], P(None, 'tp'), may hold values from -3 to 3
- gate_a_weight: bfloat16 [24, 64, 64], P('tp'), may hold values from -0.75 to 0.75
- gate_x_weight: bfloat16 [24, 64, 64], P('tp'), may hold values from -0.75 to 0.75
- decay_param: float32 [1536], P('tp'), may hold values from 3.7 to 9
- mix_out_weight: bfloat16 [1536, 2048], P('tp', 'fs'), may hold values from -0.15625 to 0.15625
- ffn2_gain: float32 [2048], replicated, may hold values from 0.1 to 1.9
- ffn2_gate: bfloat16 [2048, 5632], P('fs', 'tp'), may hold values from -0.125 to 0.125
- ffn2_up: bfloat16 [2048, 5632], P('fs', 'tp'), may hold values from -0.125 to 0.125
- ffn2_down: bfloat16 [5632, 2048], P('tp', 'fs'), may hold values from -0.078125 to 0.078125
Outputs:
- layer_out: bfloat16 [12288, 2048], P(('fs', 'tp'))
The draws below stay inside these ranges and needn't reach their ends.
All inputs are finite; a program needn't handle non-finite values.
Results may differ from the reference program's by a relative error of at most 0.017.
Values may be sent and summed in bfloat16 or wider, within the bound.
No kernel may reach another device: no remote copies, remote signals or barrier semaphores. Data moves between devices by JAX's collectives and lax.ppermute only.
A program may use at most 64 MiB of HBM per device.

```python
import jax
import jax.numpy as jnp
from jax import lax

D = 2048
FF = 5632
DR = 1536
LB = 64
WIDTH = 4
SEQ = 384
NB = 24
TOKENS = 12288
N_FS = 32
N_TP = 8


def draw_decay_param(key, part):
    first_key, second_key, third_key = jax.random.split(jax.random.fold_in(key, 17), 3)
    slow_share = 0.5
    slow = jax.random.bernoulli(first_key, slow_share, (DR,))
    fast_values = jax.random.uniform(second_key, (DR,), jnp.float32, 3.7, 4.9)
    slow_values = jax.random.uniform(third_key, (DR,), jnp.float32, 7.5, 9.0)
    return jnp.where(slow, slow_values, fast_values).astype(jnp.float32)


def block_scale(own_key, extent, pieces, low, largest):
    loudness = 1.0
    for dim, shards_of in pieces:
        draws = jax.random.uniform(jax.random.fold_in(jax.random.fold_in(own_key, 6), dim), (shards_of,), jnp.float32, low / len(pieces), largest / len(pieces))
        loudness = loudness * jnp.repeat(jnp.exp(draws), extent[dim] // shards_of).reshape((-1,) + (1,) * (len(extent) - 1 - dim))
    return loudness


def normal_values(key, dims, scale, limit, pieces=(), kind=jnp.bfloat16):
    level = block_scale(key, dims, pieces, -0.22, 0.18) if pieces else 1.0
    array = jax.random.normal(key, dims, jnp.float32) * scale * level
    return jnp.minimum(jnp.maximum(array, -limit), limit).astype(kind)


def setup_inputs(seed: int = 0) -> dict:
    key_list = jax.random.split(jax.random.key(seed), 18)
    return {
        "tokens": normal_values(key_list[0], (TOKENS, D), 1.0, 6.0, ((0, 256),)),
        "ffn1_gain": jnp.clip(1.0 + 0.18 * jax.random.normal(key_list[1], (D,), jnp.float32), 0.1, 1.9),
        "ffn1_gate": normal_values(key_list[2], (D, FF), D ** -0.5, 0.125, ((0, 32), (1, 8))),
        "ffn1_up": normal_values(key_list[3], (D, FF), D ** -0.5, 0.125, ((0, 32), (1, 8))),
        "ffn1_down": normal_values(key_list[4], (FF, D), FF ** -0.5, 0.078125, ((0, 8), (1, 32))),
        "mix_gain": jnp.clip(1.0 + 0.18 * jax.random.normal(key_list[5], (D,), jnp.float32), 0.1, 1.9),
        "lru_in_weight": normal_values(key_list[6], (D, DR), D ** -0.5, 0.125, ((0, 32), (1, 8))),
        "lru_gate_weight": normal_values(key_list[7], (D, DR), D ** -0.5, 0.125, ((0, 32), (1, 8))),
        "conv_weight": normal_values(key_list[8], (WIDTH, DR), WIDTH ** -0.5, 3.0, ((1, 8),)),
        "gate_a_weight": normal_values(key_list[9], (NB, LB, LB), LB ** -0.5, 0.75, ((0, 8),)),
        "gate_x_weight": normal_values(key_list[10], (NB, LB, LB), LB ** -0.5, 0.75, ((0, 8),)),
        "decay_param": draw_decay_param(jax.random.fold_in(key_list[17], 71), 0),
        "mix_out_weight": normal_values(key_list[12], (DR, D), DR ** -0.5, 0.15625, ((0, 8), (1, 32))),
        "ffn2_gain": jnp.clip(1.0 + 0.18 * jax.random.normal(key_list[13], (D,), jnp.float32), 0.1, 1.9),
        "ffn2_gate": normal_values(key_list[14], (D, FF), D ** -0.5, 0.125, ((0, 32), (1, 8))),
        "ffn2_up": normal_values(key_list[15], (D, FF), D ** -0.5, 0.125, ((0, 32), (1, 8))),
        "ffn2_down": normal_values(key_list[16], (FF, D), FF ** -0.5, 0.078125, ((0, 8), (1, 32))),
    }


EPS = 1e-06

def rms_rows(values, gain):
    wide = values.astype(jnp.float32)
    scale = lax.rsqrt(lax.optimization_barrier(jnp.mean(wide * wide, axis=-1, keepdims=True)) + EPS)
    return (wide * scale * gain.astype(jnp.float32)).astype(jnp.bfloat16)

def group_sums(hidden, weight):
    rows = hidden.shape[0]
    inner = hidden.shape[1] // N_TP
    hidden_groups = hidden.reshape(rows, N_TP, inner).transpose(1, 0, 2)
    weight_groups = weight.reshape(N_TP, inner, weight.shape[1])

    def add_group(total, pair):
        part = jnp.dot(pair[0], pair[1], preferred_element_type=jnp.float32).astype(jnp.bfloat16)
        return (total + lax.optimization_barrier(part).astype(jnp.float32), None)
    start = jnp.zeros((rows, weight.shape[1]), jnp.float32)
    total, _ = lax.scan(add_group, start, (hidden_groups, weight_groups))
    return total

def half_block(values, gain, gate_weight, up_weight, down_weight):
    normed = rms_rows(values, gain)
    gate = jnp.dot(normed, gate_weight, preferred_element_type=jnp.float32)
    upper = jnp.dot(normed, up_weight, preferred_element_type=jnp.float32)
    hidden = (jax.nn.silu(gate) * upper).astype(jnp.bfloat16)
    return group_sums(hidden, down_weight)

def combine(earlier, later):
    return (earlier[0] * later[0], later[0] * earlier[1] + later[1])

def reference(tokens, ffn1_gain, ffn1_gate, ffn1_up, ffn1_down, mix_gain, lru_in_weight, lru_gate_weight, conv_weight, gate_a_weight, gate_x_weight, decay_param, mix_out_weight, ffn2_gain, ffn2_gate, ffn2_up, ffn2_down):
    first = (tokens.astype(jnp.float32) + 0.5 * half_block(tokens, ffn1_gain, ffn1_gate, ffn1_up, ffn1_down)).astype(jnp.bfloat16)
    normed = rms_rows(first, mix_gain)
    lru_x = jnp.dot(normed, lru_in_weight, preferred_element_type=jnp.float32).astype(jnp.bfloat16)
    lru_gate = jnp.dot(normed, lru_gate_weight, preferred_element_type=jnp.float32).astype(jnp.bfloat16)
    seqs = lru_x.astype(jnp.float32).reshape(N_FS, SEQ, DR)
    padded = jnp.pad(seqs, ((0, 0), (WIDTH - 1, 0), (0, 0)))
    taps = conv_weight.astype(jnp.float32)
    conv = jnp.zeros((N_FS, SEQ, DR), jnp.float32)
    for offset in range(WIDTH):
        conv = conv + taps[offset] * padded[:, WIDTH - 1 - offset:WIDTH - 1 - offset + SEQ]
    conv_low = conv.astype(jnp.bfloat16).astype(jnp.float32)
    blocks = conv_low.reshape(N_FS, SEQ, NB, LB)
    recall = jax.nn.sigmoid(jnp.einsum('nsbi,bij->nsbj', blocks, gate_a_weight.astype(jnp.float32)).reshape(N_FS, SEQ, DR))
    admit = jax.nn.sigmoid(jnp.einsum('nsbi,bij->nsbj', blocks, gate_x_weight.astype(jnp.float32)).reshape(N_FS, SEQ, DR))
    log_keep = -8.0 * recall * jax.nn.softplus(-decay_param)
    drive = jnp.sqrt(-jnp.expm1(2.0 * log_keep)) * admit * conv_low
    _, state = lax.associative_scan(combine, (jnp.exp(log_keep), drive), axis=1)
    mixed = (state.reshape(TOKENS, DR) * jax.nn.gelu(lru_gate.astype(jnp.float32))).astype(jnp.bfloat16)
    second = (first.astype(jnp.float32) + group_sums(mixed, mix_out_weight)).astype(jnp.bfloat16)
    return (second.astype(jnp.float32) + 0.5 * half_block(second, ffn2_gain, ffn2_gate, ffn2_up, ffn2_down)).astype(jnp.bfloat16)
```

```python
import jax
import jax.numpy as jnp
from jax import lax
from jax.experimental import pallas as pl
from jax.experimental.pallas import tpu as pltpu
from jax.sharding import Mesh
from jax.sharding import PartitionSpec as P

FS = ("fs_0", "fs_1")
FS_TP = ("fs_0", "fs_1", "tp")

EPS = 1e-06
LANES = 128
SHARD = 64
HALF = 64


def rms_rows(values, gain):
    wide = values.astype(jnp.float32)
    scale = lax.rsqrt(jnp.mean(wide * wide, axis=-1, keepdims=True) + EPS)
    return (wide * scale * gain).astype(jnp.bfloat16)


def gather_rows(values):
    copies = jnp.broadcast_to(values, (lax.axis_size("tp"), *values.shape))
    arrived = lax.all_to_all(copies, "tp", split_axis=0, concat_axis=0, tiled=True)
    return arrived.reshape(-1, values.shape[-1])


def reduce_rows(terms):
    blocks = terms.reshape(lax.axis_size("tp"), -1, terms.shape[-1])
    arrived = lax.all_to_all(blocks, "tp", split_axis=0, concat_axis=0, tiled=True)
    return arrived.astype(jnp.float32).sum(axis=0)


def tiles_of(weight):
    return [weight[:, k : k + LANES] for k in range(0, weight.shape[1], LANES)]


def paired_tiles(first, second):
    whole = first.shape[1] // LANES * LANES
    ends = jnp.concatenate([first[:, whole:], second[:, whole:]], axis=1)
    return tiles_of(first[:, :whole]) + tiles_of(second[:, :whole]) + [ends]


def gather_tiles(tiles):
    packed = jnp.concatenate(tiles, axis=0)
    full = lax.all_gather(packed, FS, axis=0, tiled=True)
    return full.reshape(-1, len(tiles), SHARD, LANES)


def nt_dot(a, b):
    return lax.dot_general(a, b, (((1,), (1,)), ((), ())), preferred_element_type=jnp.float32)


def flat(ref, k):
    block = ref[:, k]
    return block.reshape(-1, LANES)


def ffn_kernel(rows_ref, first_ref, second_ref, down_ref, out_ref, hidden_ref):
    step = pl.program_id(0)
    last = pl.num_programs(0) - 1

    @pl.when(step < last)
    def _():
        both = jnp.concatenate([flat(first_ref, 0), flat(second_ref, 0)], axis=1)
        z = jnp.dot(rows_ref[...], both, preferred_element_type=jnp.float32)
        gate = z[:, :LANES]
        hidden = gate * jax.nn.sigmoid(gate) * z[:, LANES:]
        at = pl.multiple_of(step * LANES, LANES)
        hidden_ref[:, pl.ds(at, LANES)] = hidden.astype(jnp.bfloat16)

    @pl.when(step == last)
    def _():
        z = jnp.dot(rows_ref[...], flat(first_ref, 0), preferred_element_type=jnp.float32)
        hidden = z * jax.nn.sigmoid(z) * pltpu.roll(z, HALF, 1)
        lane = lax.broadcasted_iota(jnp.int32, z.shape, 1)
        hidden = jnp.where(lane < HALF, hidden, 0.0)
        tiles = hidden_ref.shape[1] // LANES
        hidden_ref[:, (tiles - 1) * LANES :] = hidden.astype(jnp.bfloat16)
        shards = 256 // SHARD
        for n in range(down_ref.shape[0] // shards):
            own = slice(n * shards, (n + 1) * shards)
            down = jnp.concatenate(
                [down_ref[own, k].reshape(-1, LANES) for k in range(tiles)], axis=1
            )
            out_ref[:, n * 256 : (n + 1) * 256] = nt_dot(hidden_ref[...], down).astype(
                jnp.bfloat16
            )


def ffn_terms(rows, packed):
    shards = packed.shape[0]
    length, width = rows.shape
    whole = lambda j: (0, 0)
    return pl.pallas_call(
        ffn_kernel,
        grid=(6,),
        in_specs=[
            pl.BlockSpec((length, width), whole),
            pl.BlockSpec((shards, 1, SHARD, LANES), lambda j: (0, jnp.where(j < 5, 6 + j, 16), 0, 0)),
            pl.BlockSpec((shards, 1, SHARD, LANES), lambda j: (0, jnp.minimum(11 + j, 15), 0, 0)),
            pl.BlockSpec((shards, 6, SHARD, LANES), lambda j: (0, 0, 0, 0)),
        ],
        out_specs=pl.BlockSpec((length, width), whole),
        out_shape=jax.ShapeDtypeStruct((length, width), jnp.bfloat16),
        scratch_shapes=[pltpu.VMEM((length, 6 * LANES), jnp.bfloat16)],
        compiler_params=pltpu.CompilerParams(vmem_limit_bytes=40 << 20),
        name="ffn",
    )(rows, packed, packed, packed)


def shifted(values, by, fill):
    row = lax.broadcasted_iota(jnp.int32, values.shape, 0)
    return jnp.where(row >= by, pltpu.roll(values, by, 0), fill)


def minus_expm1(x):
    series = 1.0 + x / 8.0
    for k in range(7, 1, -1):
        series = 1.0 + (x / k) * series
    return jnp.where(x > -0.5, -x * series, 1.0 - jnp.exp(x))


def scanned(keep, drive):
    by = 1
    while by < keep.shape[0]:
        drive = keep * shifted(drive, by, 0.0) + drive
        keep = keep * shifted(keep, by, 1.0)
        by *= 2
    return drive


def mixer_kernel(
    rows_ref, x_ref, gate_ref, ends_ref, out0_ref, out1_ref, taps_ref, a_ref, b_ref, rate_ref, out_ref
):
    rows = rows_ref[...]
    z = jnp.dot(
        rows, jnp.concatenate([flat(x_ref, 0), flat(gate_ref, 0)], axis=1), preferred_element_type=jnp.float32
    )
    ends = jnp.dot(rows, flat(ends_ref, 0), preferred_element_type=jnp.float32)
    lane = lax.broadcasted_iota(jnp.int32, ends.shape, 1)
    groups = (
        (z[:, :LANES], z[:, LANES:]),
        (jnp.where(lane < HALF, ends, 0.0), pltpu.roll(ends, HALF, 1)),
    )
    mixed = []
    for g, (lru_x, lru_gate) in enumerate(groups):
        lru_x = lru_x.astype(jnp.bfloat16).astype(jnp.float32)
        lru_gate = lru_gate.astype(jnp.bfloat16).astype(jnp.float32)
        own = slice(g * LANES, (g + 1) * LANES)
        taps = taps_ref[:, own]
        conv = taps[0:1] * lru_x
        for k in range(1, 4):
            conv = conv + taps[k : k + 1] * shifted(lru_x, k, 0.0)
        low = conv.astype(jnp.bfloat16)
        recall = jax.nn.sigmoid(jnp.dot(low, a_ref[g], preferred_element_type=jnp.float32))
        admit = jax.nn.sigmoid(jnp.dot(low, b_ref[g], preferred_element_type=jnp.float32))
        log_keep = recall * rate_ref[:, own]
        drive = jnp.sqrt(minus_expm1(2.0 * log_keep)) * admit * low.astype(jnp.float32)
        state = scanned(jnp.exp(log_keep), drive)
        mixed.append((state * jax.nn.gelu(lru_gate)).astype(jnp.bfloat16))
    shards = 256 // SHARD
    short = mixed[1][:, :HALF]
    for n in range(out0_ref.shape[0] // shards):
        own = slice(n * shards, (n + 1) * shards)
        terms = nt_dot(mixed[0], out0_ref[own, 0].reshape(-1, LANES))
        terms = terms + nt_dot(short, out1_ref[own, 0].reshape(-1, LANES)[:, HALF:])
        out_ref[:, n * 256 : (n + 1) * 256] = terms.astype(jnp.bfloat16)


def paired_blocks(blocks):
    zero = jnp.zeros_like(blocks[0])
    top = jnp.concatenate(
        [jnp.concatenate([blocks[0], zero], 1), jnp.concatenate([zero, blocks[1]], 1)], 0
    )
    end = jnp.concatenate(
        [jnp.concatenate([blocks[2], zero], 1), jnp.concatenate([zero, zero], 1)], 0
    )
    return jnp.stack([top, end])


def mixer_terms(rows, packed, conv_weight, gate_a_weight, gate_x_weight, decay_param):
    shards = packed.shape[0]
    length, width = rows.shape
    pad = ((0, 0), (0, HALF))
    taps = jnp.pad(conv_weight.astype(jnp.float32), pad)
    rate = jnp.pad(-8.0 * jax.nn.softplus(-decay_param)[None], pad)
    tile = lambda k: pl.BlockSpec((shards, 1, SHARD, LANES), lambda j: (0, k, 0, 0))
    whole = lambda *shape: pl.BlockSpec(shape, lambda j: (0,) * len(shape))
    return pl.pallas_call(
        mixer_kernel,
        grid=(1,),
        in_specs=[
            whole(length, width),
            tile(17),
            tile(18),
            tile(19),
            tile(20),
            tile(5),
            whole(4, 2 * LANES),
            whole(2, LANES, LANES),
            whole(2, LANES, LANES),
            whole(1, 2 * LANES),
        ],
        out_specs=whole(length, width),
        out_shape=jax.ShapeDtypeStruct((length, width), jnp.bfloat16),
        compiler_params=pltpu.CompilerParams(vmem_limit_bytes=40 << 20),
        name="mixer",
    )(
        rows,
        packed,
        packed,
        packed,
        packed,
        packed,
        taps,
        paired_blocks(gate_a_weight),
        paired_blocks(gate_x_weight),
        rate,
    )


def body(
    tokens,
    ffn1_gain,
    ffn1_gate,
    ffn1_up,
    ffn1_down,
    mix_gain,
    lru_in_weight,
    lru_gate_weight,
    conv_weight,
    gate_a_weight,
    gate_x_weight,
    decay_param,
    mix_out_weight,
    ffn2_gain,
    ffn2_gate,
    ffn2_up,
    ffn2_down,
):
    down = ffn1_down.T
    out = mix_out_weight.T
    packed1 = gather_tiles(
        tiles_of(down[:, :640])
        + [jnp.concatenate([down[:, 640:], out[:, LANES:]], axis=1)]
        + paired_tiles(ffn1_gate, ffn1_up)
        + paired_tiles(lru_in_weight, lru_gate_weight)
        + [out[:, :LANES]]
    )
    down = ffn2_down.T
    packed2 = gather_tiles(
        tiles_of(down[:, :640])
        + [jnp.pad(down[:, 640:], ((0, 0), (0, HALF)))]
        + paired_tiles(ffn2_gate, ffn2_up)
    )
    rows = gather_rows(rms_rows(tokens, ffn1_gain))
    terms = ffn_terms(rows, packed1)
    first = (tokens.astype(jnp.float32) + 0.5 * reduce_rows(terms)).astype(jnp.bfloat16)
    rows = gather_rows(rms_rows(first, mix_gain))
    terms = mixer_terms(rows, packed1, conv_weight, gate_a_weight, gate_x_weight, decay_param)
    second = (first.astype(jnp.float32) + reduce_rows(terms)).astype(jnp.bfloat16)
    rows = gather_rows(rms_rows(second, ffn2_gain))
    terms = ffn_terms(rows, packed2)
    return (second.astype(jnp.float32) + 0.5 * reduce_rows(terms)).astype(jnp.bfloat16)


def solution(mesh):
    split = Mesh(mesh.devices.reshape(8, 4, mesh.shape["tp"]), ("fs_0", "fs_1", "tp"))
    placed = (
        P(FS_TP, None),
        P(),
        P(FS, "tp"),
        P(FS, "tp"),
        P("tp", FS),
        P(),
        P(FS, "tp"),
        P(FS, "tp"),
        P(None, "tp"),
        P("tp", None, None),
        P("tp", None, None),
        P("tp"),
        P("tp", FS),
        P(),
        P(FS, "tp"),
        P(FS, "tp"),
        P("tp", FS),
    )
    return jax.shard_map(
        body, mesh=split, in_specs=placed, out_specs=P(FS_TP, None), check_vma=False
    )
```

```python
import jax
import jax.numpy as jnp
from jax import lax
from jax.experimental import pallas as pl
from jax.experimental.pallas import tpu as pltpu
from jax.sharding import Mesh
from jax.sharding import PartitionSpec as P

FS = ("z", "y")
TP = ("x", "c")
FS_TP = ("z", "y", "x", "c")

EPS = 1e-06
LANES = 128
SHARD = 64
HALF = 64


def moved(value, axis, by):
    count = lax.axis_size(axis)
    return lax.ppermute(value, axis, [(i, (i - by) % count) for i in range(count)])


def in_hbm(value):
    return pltpu.with_memory_space_constraint(value, pltpu.HBM)


def whole(*shape):
    return pl.BlockSpec(shape, lambda *_: (0,) * len(shape))


def norm_of(wide, gain):
    scale = lax.rsqrt(jnp.mean(wide * wide, axis=-1, keepdims=True) + EPS)
    return (wide * scale * gain).astype(jnp.bfloat16)


def norm_kernel(rows_ref, gain_ref, out_ref):
    out_ref[...] = norm_of(rows_ref[...].astype(jnp.float32), gain_ref[...])


def rms_rows(values, gain):
    return pl.pallas_call(
        norm_kernel,
        out_shape=jax.ShapeDtypeStruct(values.shape, jnp.bfloat16),
        name="norm",
    )(values, gain[None])


def gather_rows(own):
    near = moved(own, "x", 1)
    far = moved(own, "x", 3)
    across = moved(own, "x", 2)
    mine = jnp.concatenate([own, near, across, far], axis=0)
    return mine, moved(mine, "c", 1)


def pair_sum_kernel(mine_ref, other_ref, *out_refs):
    rows = out_refs[0].shape[0]
    for n, out_ref in enumerate(out_refs):
        own = slice(n * rows, (n + 1) * rows)
        out_ref[...] = (
            mine_ref[own].astype(jnp.float32) + other_ref[own].astype(jnp.float32)
        ).astype(jnp.bfloat16)


def sent_sums(terms):
    mine, other = terms
    other = moved(other, "c", 1)
    count = lax.axis_size("x")
    shape = jax.ShapeDtypeStruct((mine.shape[0] // count, mine.shape[1]), jnp.bfloat16)
    sums = pl.pallas_call(pair_sum_kernel, out_shape=[shape] * count, name="pair_sum")(mine, other)
    return [sums[0]] + [moved(sums[n], "x", -n) for n in range(1, count)]


def combine_kernel(half, base_ref, a_ref, b_ref, c_ref, d_ref, *refs):
    total = a_ref[...].astype(jnp.float32) + b_ref[...].astype(jnp.float32)
    total = total + c_ref[...].astype(jnp.float32) + d_ref[...].astype(jnp.float32)
    if half:
        total = 0.5 * total
    result = (base_ref[...].astype(jnp.float32) + total).astype(jnp.bfloat16)
    if len(refs) == 1:
        refs[0][...] = result
    else:
        gain_ref, out_ref, norm_ref = refs
        out_ref[...] = result
        norm_ref[...] = norm_of(result.astype(jnp.float32), gain_ref[...])


def combined(base, sums, half, gain=None):
    shape = jax.ShapeDtypeStruct(base.shape, jnp.bfloat16)
    extra = () if gain is None else (gain[None],)
    outs = [shape] if gain is None else [shape, shape]
    return pl.pallas_call(
        lambda *refs: combine_kernel(half, *refs), out_shape=outs, name="combine"
    )(base, *sums, *extra)


def pack_kernel(plan, *refs):
    *in_refs, out_ref = refs
    for n, parts in enumerate(plan):
        pieces = [in_refs[which][:, at : at + size] for which, at, size in parts]
        if len(pieces) == 2:
            low, high = (p.astype(jnp.float32) for p in pieces)
            tile = jnp.concatenate([low, high], axis=1).astype(jnp.bfloat16)
        else:
            tile = pieces[0]
        if tile.shape[1] < LANES:
            out_ref[n * SHARD : (n + 1) * SHARD] = jnp.zeros((SHARD, LANES), jnp.bfloat16)
        out_ref[n * SHARD : (n + 1) * SHARD, : tile.shape[1]] = tile


def packed_tiles(plan, arrays):
    return pl.pallas_call(
        lambda *refs: pack_kernel(plan, *refs),
        out_shape=jax.ShapeDtypeStruct((len(plan) * SHARD, LANES), jnp.bfloat16),
        name="pack",
    )(*arrays)


def full_tiles(which, count):
    return [((which, k * LANES, LANES),) for k in range(count)]


def gather_tiles(plan, arrays):
    packed = packed_tiles(plan, arrays)
    full = lax.all_gather(packed, FS, axis=0, tiled=True)
    return in_hbm(full.reshape(-1, len(plan), SHARD, LANES))


def nt_dot(a, b):
    return lax.dot_general(a, b, (((1,), (1,)), ((), ())), preferred_element_type=jnp.float32)


def flat(ref, k):
    block = ref[:, k]
    return block.reshape(-1, LANES)


def ffn_kernel(
    mine_ref, other_ref, first_ref, second_ref, down_ref, out_mine_ref, out_other_ref, hidden_ref, rows_ref
):
    step = pl.program_id(0)
    last = pl.num_programs(0) - 1
    half = mine_ref.shape[0]

    @pl.when(step == 0)
    def _():
        rows_ref[:half] = mine_ref[...]
        rows_ref[half:] = other_ref[...]

    @pl.when(step < last)
    def _():
        both = jnp.concatenate([flat(first_ref, 0), flat(second_ref, 0)], axis=1)
        z = jnp.dot(rows_ref[...], both, preferred_element_type=jnp.float32)
        gate = z[:, :LANES]
        hidden = gate * jax.nn.sigmoid(gate) * z[:, LANES:]
        at = pl.multiple_of(step * LANES, LANES)
        hidden_ref[:, pl.ds(at, LANES)] = hidden.astype(jnp.bfloat16)

    @pl.when(step == last)
    def _():
        z = jnp.dot(rows_ref[...], flat(first_ref, 0), preferred_element_type=jnp.float32)
        hidden = z * jax.nn.sigmoid(z) * pltpu.roll(z, HALF, 1)
        lane = lax.broadcasted_iota(jnp.int32, z.shape, 1)
        hidden = jnp.where(lane < HALF, hidden, 0.0)
        tiles = hidden_ref.shape[1] // LANES
        hidden_ref[:, (tiles - 1) * LANES :] = hidden.astype(jnp.bfloat16)
        shards = 256 // SHARD
        for n in range(down_ref.shape[0] // shards):
            own = slice(n * shards, (n + 1) * shards)
            down = jnp.concatenate(
                [down_ref[own, k].reshape(-1, LANES) for k in range(tiles)], axis=1
            )
            terms = nt_dot(hidden_ref[...], down).astype(jnp.bfloat16)
            out_mine_ref[:, n * 256 : (n + 1) * 256] = terms[:half]
            out_other_ref[:, n * 256 : (n + 1) * 256] = terms[half:]


def ffn_terms(rows, packed):
    shards = packed.shape[0]
    half, width = rows[0].shape
    return pl.pallas_call(
        ffn_kernel,
        grid=(6,),
        in_specs=[
            whole(half, width),
            whole(half, width),
            pl.BlockSpec((shards, 1, SHARD, LANES), lambda j: (0, jnp.where(j < 5, 6 + j, 16), 0, 0)),
            pl.BlockSpec((shards, 1, SHARD, LANES), lambda j: (0, jnp.minimum(11 + j, 15), 0, 0)),
            pl.BlockSpec((shards, 6, SHARD, LANES), lambda j: (0, 0, 0, 0)),
        ],
        out_specs=[whole(half, width)] * 2,
        out_shape=[jax.ShapeDtypeStruct((half, width), jnp.bfloat16)] * 2,
        scratch_shapes=[
            pltpu.VMEM((2 * half, 6 * LANES), jnp.bfloat16),
            pltpu.VMEM((2 * half, width), jnp.bfloat16),
        ],
        compiler_params=pltpu.CompilerParams(vmem_limit_bytes=40 << 20),
        name="ffn",
    )(*rows, packed, packed, packed)


def shifted(values, by, fill):
    row = lax.broadcasted_iota(jnp.int32, values.shape, 0)
    return jnp.where(row >= by, pltpu.roll(values, by, 0), fill)


def minus_expm1(x):
    series = 1.0 + x / 8.0
    for k in range(7, 1, -1):
        series = 1.0 + (x / k) * series
    return jnp.where(x > -0.5, -x * series, 1.0 - jnp.exp(x))


def scanned(keep, drive):
    by = 1
    while by < keep.shape[0]:
        drive = keep * shifted(drive, by, 0.0) + drive
        keep = keep * shifted(keep, by, 1.0)
        by *= 2
    return drive


def mixer_kernel(
    mine_ref,
    other_ref,
    x_ref,
    gate_ref,
    ends_ref,
    out0_ref,
    out1_ref,
    taps_ref,
    a_ref,
    b_ref,
    rate_ref,
    out_mine_ref,
    out_other_ref,
    order_ref,
):
    half = mine_ref.shape[0]
    chips = lax.axis_size("x")
    block = half // chips
    x = lax.axis_index("x")
    core = lax.axis_index("c")
    weights = jnp.concatenate([flat(x_ref, 0), flat(gate_ref, 0), flat(ends_ref, 0)], axis=1)
    places = []
    for n, ref in enumerate((mine_ref, other_ref)):
        part = jnp.dot(ref[...], weights, preferred_element_type=jnp.float32)
        for k in range(chips):
            chip = lax.rem(x + k, chips)
            which = core if n == 0 else 1 - core
            place = pl.multiple_of((chip * 2 + which) * block, block)
            places.append(place)
            order_ref[pl.ds(place, block), :] = part[k * block : (k + 1) * block]
    z = order_ref[:, : 2 * LANES]
    ends = order_ref[:, 2 * LANES :]
    lane = lax.broadcasted_iota(jnp.int32, ends.shape, 1)
    groups = (
        (z[:, :LANES], z[:, LANES:]),
        (jnp.where(lane < HALF, ends, 0.0), pltpu.roll(ends, HALF, 1)),
    )
    mixed = []
    for g, (lru_x, lru_gate) in enumerate(groups):
        lru_x = lru_x.astype(jnp.bfloat16).astype(jnp.float32)
        lru_gate = lru_gate.astype(jnp.bfloat16).astype(jnp.float32)
        own = slice(g * LANES, (g + 1) * LANES)
        taps = taps_ref[:, own]
        conv = taps[0:1] * lru_x
        for k in range(1, 4):
            conv = conv + taps[k : k + 1] * shifted(lru_x, k, 0.0)
        low = conv.astype(jnp.bfloat16)
        recall = jax.nn.sigmoid(jnp.dot(low, a_ref[g], preferred_element_type=jnp.float32))
        admit = jax.nn.sigmoid(jnp.dot(low, b_ref[g], preferred_element_type=jnp.float32))
        log_keep = recall * rate_ref[:, own]
        drive = jnp.sqrt(minus_expm1(2.0 * log_keep)) * admit * low.astype(jnp.float32)
        state = scanned(jnp.exp(log_keep), drive)
        mixed.append(state * jax.nn.gelu(lru_gate))
    for g in range(2):
        order_ref[:, g * LANES : (g + 1) * LANES] = mixed[g]
    mixed = jnp.concatenate([order_ref[pl.ds(p, block), : 2 * LANES] for p in places], axis=0)
    mixed = mixed.astype(jnp.bfloat16)
    full = mixed[:, :LANES]
    short = mixed[:, LANES : LANES + HALF]
    shards = 256 // SHARD
    for n in range(out0_ref.shape[0] // shards):
        own = slice(n * shards, (n + 1) * shards)
        terms = nt_dot(full, out0_ref[own, 0].reshape(-1, LANES))
        terms = terms + nt_dot(short, out1_ref[own, 0].reshape(-1, LANES)[:, HALF:])
        terms = terms.astype(jnp.bfloat16)
        out_mine_ref[:, n * 256 : (n + 1) * 256] = terms[:half]
        out_other_ref[:, n * 256 : (n + 1) * 256] = terms[half:]


def paired_blocks(blocks):
    zero = jnp.zeros_like(blocks[0])
    top = jnp.concatenate(
        [jnp.concatenate([blocks[0], zero], 1), jnp.concatenate([zero, blocks[1]], 1)], 0
    )
    end = jnp.concatenate(
        [jnp.concatenate([blocks[2], zero], 1), jnp.concatenate([zero, zero], 1)], 0
    )
    return jnp.stack([top, end])


def mixer_terms(rows, packed, conv_weight, gate_a_weight, gate_x_weight, decay_param):
    shards = packed.shape[0]
    half, width = rows[0].shape
    pad = ((0, 0), (0, HALF))
    taps = jnp.pad(conv_weight.astype(jnp.float32), pad)
    rate = jnp.pad(-8.0 * jax.nn.softplus(-decay_param)[None], pad)
    tile = lambda k: pl.BlockSpec((shards, 1, SHARD, LANES), lambda j: (0, k, 0, 0))
    return pl.pallas_call(
        mixer_kernel,
        grid=(1,),
        in_specs=[
            whole(half, width),
            whole(half, width),
            tile(17),
            tile(18),
            tile(19),
            tile(20),
            tile(5),
            whole(4, 2 * LANES),
            whole(2, LANES, LANES),
            whole(2, LANES, LANES),
            whole(1, 2 * LANES),
        ],
        out_specs=[whole(half, width)] * 2,
        out_shape=[jax.ShapeDtypeStruct((half, width), jnp.bfloat16)] * 2,
        scratch_shapes=[pltpu.VMEM((2 * half, 3 * LANES), jnp.float32)],
        compiler_params=pltpu.CompilerParams(vmem_limit_bytes=40 << 20),
        name="mixer",
    )(
        *rows,
        packed,
        packed,
        packed,
        packed,
        packed,
        taps,
        paired_blocks(gate_a_weight),
        paired_blocks(gate_x_weight),
        rate,
    )


def body(
    tokens,
    ffn1_gain,
    ffn1_gate,
    ffn1_up,
    ffn1_down,
    mix_gain,
    lru_in_weight,
    lru_gate_weight,
    conv_weight,
    gate_a_weight,
    gate_x_weight,
    decay_param,
    mix_out_weight,
    ffn2_gain,
    ffn2_gate,
    ffn2_up,
    ffn2_down,
):
    plan = full_tiles(0, 5) + [((0, 640, HALF), (1, LANES, HALF))]
    plan += full_tiles(2, 5) + full_tiles(3, 5) + [((2, 640, HALF), (3, 640, HALF))]
    plan += full_tiles(4, 1) + full_tiles(5, 1) + [((4, LANES, HALF), (5, LANES, HALF))]
    plan += full_tiles(1, 1)
    packed1 = gather_tiles(
        plan, [ffn1_down.T, mix_out_weight.T, ffn1_gate, ffn1_up, lru_in_weight, lru_gate_weight]
    )
    plan = full_tiles(0, 5) + [((0, 640, HALF),)]
    plan += full_tiles(1, 5) + full_tiles(2, 5) + [((1, 640, HALF), (2, 640, HALF))]
    packed2 = gather_tiles(plan, [ffn2_down.T, ffn2_gate, ffn2_up])
    rows = gather_rows(rms_rows(tokens, ffn1_gain))
    sums = sent_sums(ffn_terms(rows, packed1))
    first, normed = combined(tokens, sums, True, mix_gain)
    rows = gather_rows(normed)
    sums = sent_sums(
        mixer_terms(rows, packed1, conv_weight, gate_a_weight, gate_x_weight, decay_param)
    )
    second, normed = combined(first, sums, False, ffn2_gain)
    rows = gather_rows(normed)
    sums = sent_sums(ffn_terms(rows, packed2))
    return combined(second, sums, True)[0]


def solution(mesh):
    split = Mesh(mesh.devices.reshape(8, 4, 4, 2), FS_TP)
    placed = (
        P(FS_TP, None),
        P(),
        P(FS, TP),
        P(FS, TP),
        P(TP, FS),
        P(),
        P(FS, TP),
        P(FS, TP),
        P(None, TP),
        P(TP, None, None),
        P(TP, None, None),
        P(TP),
        P(TP, FS),
        P(),
        P(FS, TP),
        P(FS, TP),
        P(TP, FS),
    )
    return jax.shard_map(
        body, mesh=split, in_specs=placed, out_specs=P(FS_TP, None), check_vma=False
    )
```

```python
import jax
import jax.numpy as jnp
from jax import lax
from jax.experimental import pallas as pl
from jax.experimental.pallas import tpu as pltpu
from jax.sharding import Mesh
from jax.sharding import PartitionSpec as P

FS = ("z", "y")
TP = ("x", "c")
FS_TP = ("z", "y", "x", "c")

EPS = 1e-06
LANES = 128
SHARD = 64
HALF = 64


def moved(value, axis, by):
    count = lax.axis_size(axis)
    return lax.ppermute(value, axis, [(i, (i - by) % count) for i in range(count)])


def in_hbm(value):
    return pltpu.with_memory_space_constraint(value, pltpu.HBM)


def in_vmem(*values):
    return tuple(pltpu.with_memory_space_constraint(v, pltpu.VMEM) for v in values)


def whole(*shape):
    return pl.BlockSpec(shape, lambda *_: (0,) * len(shape))


def norm_of(wide, gain):
    scale = lax.rsqrt(jnp.mean(wide * wide, axis=-1, keepdims=True) + EPS)
    return (wide * scale * gain).astype(jnp.bfloat16)


def norm_kernel(rows_ref, gain_ref, out_ref):
    out_ref[...] = norm_of(rows_ref[...].astype(jnp.float32), gain_ref[...])


def rms_rows(values, gain):
    return pl.pallas_call(
        norm_kernel,
        out_shape=pltpu.VMEM(values.shape, jnp.bfloat16),
        name="norm",
    )(values, gain[None])


def gather_rows(own):
    near = moved(own, "x", 1)
    far = moved(own, "x", 3)
    across = moved(own, "x", 2)
    mine = jnp.concatenate([own, near, across, far], axis=0)
    return mine, moved(mine, "c", 1)


def pair_sum_kernel(mine_ref, other_ref, *out_refs):
    rows = out_refs[0].shape[0]
    for n, out_ref in enumerate(out_refs):
        own = slice(n * rows, (n + 1) * rows)
        out_ref[...] = (
            mine_ref[own].astype(jnp.float32) + other_ref[own].astype(jnp.float32)
        ).astype(jnp.bfloat16)


def sent_sums(terms):
    mine, other = terms
    other = moved(other, "c", 1)
    count = lax.axis_size("x")
    shape = pltpu.VMEM((mine.shape[0] // count, mine.shape[1]), jnp.bfloat16)
    sums = pl.pallas_call(pair_sum_kernel, out_shape=[shape] * count, name="pair_sum")(
        *in_vmem(mine, other)
    )
    return [sums[0]] + [moved(sums[n], "x", -n) for n in range(1, count)]


def combine_kernel(half, base_ref, a_ref, b_ref, c_ref, d_ref, *refs):
    total = a_ref[...].astype(jnp.float32) + b_ref[...].astype(jnp.float32)
    total = total + c_ref[...].astype(jnp.float32) + d_ref[...].astype(jnp.float32)
    if half:
        total = 0.5 * total
    result = (base_ref[...].astype(jnp.float32) + total).astype(jnp.bfloat16)
    if len(refs) == 1:
        refs[0][...] = result
    else:
        gain_ref, out_ref, norm_ref = refs
        out_ref[...] = result
        norm_ref[...] = norm_of(result.astype(jnp.float32), gain_ref[...])


def combined(base, sums, half, gain=None):
    shape = pltpu.VMEM(base.shape, jnp.bfloat16)
    extra = () if gain is None else (gain[None],)
    outs = [jax.ShapeDtypeStruct(base.shape, jnp.bfloat16)] if gain is None else [shape, shape]
    return pl.pallas_call(
        lambda *refs: combine_kernel(half, *refs), out_shape=outs, name="combine"
    )(*in_vmem(base, *sums, *extra))


def pack_kernel(plan, counts, *refs):
    in_refs, out_refs = refs[: -len(counts)], refs[-len(counts) :]
    places = [(ref, k) for ref, count in zip(out_refs, counts) for k in range(count)]
    for (out_ref, n), parts in zip(places, plan):
        pieces = [in_refs[which][:, at : at + size] for which, at, size in parts]
        if len(pieces) == 2:
            low, high = (p.astype(jnp.float32) for p in pieces)
            tile = jnp.concatenate([low, high], axis=1).astype(jnp.bfloat16)
        else:
            tile = pieces[0]
        if tile.shape[1] < LANES:
            out_ref[n] = jnp.zeros((SHARD, LANES), jnp.bfloat16)
        out_ref[n, :, : tile.shape[1]] = tile


def packed_tiles(plan, arrays, counts):
    return pl.pallas_call(
        lambda *refs: pack_kernel(plan, counts, *refs),
        out_shape=[jax.ShapeDtypeStruct((n, SHARD, LANES), jnp.bfloat16) for n in counts],
        name="pack",
    )(*arrays)


def full_tiles(which, count):
    return [((which, k * LANES, LANES),) for k in range(count)]


def gather_tiles(plan, arrays):
    (packed,) = packed_tiles(plan, arrays, (len(plan),))
    full = lax.all_gather(packed.reshape(-1, LANES), FS, axis=0, tiled=True)
    return in_hbm(full.reshape(-1, len(plan), SHARD, LANES))


def spread_z_last(own):
    block = jnp.stack([own, moved(own, "y", 1), moved(own, "y", 2), moved(own, "y", 3)])
    pieces = [(block, [(0, k) for k in range(4)])]
    up = down = block
    for far in range(1, 4):
        up = moved(up, "z", 1)
        down = moved(down, "z", -1)
        pieces.append((up, [(far, k) for k in range(4)]))
        pieces.append((down, [(8 - far, k) for k in range(4)]))
    pieces.append((moved(up[:2], "z", 1), [(4, 0), (4, 1)]))
    pieces.append((moved(down[2:], "z", -1), [(4, 2), (4, 3)]))
    return pieces


def spread_y_last(own):
    parts = {0: own}
    for far in range(1, 4):
        parts[far] = moved(parts[far - 1], "z", 1)
        parts[8 - far] = moved(parts[(9 - far) % 8], "z", -1)
    parts[4] = moved(parts[3], "z", 1)
    block = jnp.stack([parts[n] for n in range(8)])
    up = moved(block, "y", 1)
    down = moved(block, "y", -1)
    return [
        (block, [(n, 0) for n in range(8)]),
        (up, [(n, 1) for n in range(8)]),
        (down, [(n, 3) for n in range(8)]),
        (moved(up[:4], "y", 1), [(n, 2) for n in range(4)]),
        (moved(down[4:], "y", -1), [(n, 2) for n in range(4, 8)]),
    ]


def nt_dot(a, b):
    return lax.dot_general(a, b, (((1,), (1,)), ((), ())), preferred_element_type=jnp.float32)


def flat(ref, k):
    block = ref[:, k]
    return block.reshape(-1, LANES)


def ffn_kernel(
    mine_ref, other_ref, first_ref, second_ref, down_ref, out_mine_ref, out_other_ref, hidden_ref, rows_ref
):
    step = pl.program_id(0)
    last = pl.num_programs(0) - 1
    half = mine_ref.shape[0]

    @pl.when(step == 0)
    def _():
        rows_ref[:half] = mine_ref[...]
        rows_ref[half:] = other_ref[...]

    @pl.when(step < last)
    def _():
        both = jnp.concatenate([flat(first_ref, 0), flat(second_ref, 0)], axis=1)
        z = jnp.dot(rows_ref[...], both, preferred_element_type=jnp.float32)
        gate = z[:, :LANES]
        hidden = gate * jax.nn.sigmoid(gate) * z[:, LANES:]
        at = pl.multiple_of(step * LANES, LANES)
        hidden_ref[:, pl.ds(at, LANES)] = hidden.astype(jnp.bfloat16)

    @pl.when(step == last)
    def _():
        z = jnp.dot(rows_ref[...], flat(first_ref, 0), preferred_element_type=jnp.float32)
        hidden = z * jax.nn.sigmoid(z) * pltpu.roll(z, HALF, 1)
        lane = lax.broadcasted_iota(jnp.int32, z.shape, 1)
        hidden = jnp.where(lane < HALF, hidden, 0.0)
        tiles = hidden_ref.shape[1] // LANES
        hidden_ref[:, (tiles - 1) * LANES :] = hidden.astype(jnp.bfloat16)
        shards = 256 // SHARD
        for n in range(down_ref.shape[0] // shards):
            own = slice(n * shards, (n + 1) * shards)
            down = jnp.concatenate(
                [down_ref[own, k].reshape(-1, LANES) for k in range(tiles)], axis=1
            )
            terms = nt_dot(hidden_ref[...], down).astype(jnp.bfloat16)
            out_mine_ref[:, n * 256 : (n + 1) * 256] = terms[:half]
            out_other_ref[:, n * 256 : (n + 1) * 256] = terms[half:]


def first_ffn_kernel(places, counts, *refs):
    mine_ref, other_ref = refs[:2]
    count = sum(len(p) for p in places)
    piece_refs = refs[2 : 2 + count]
    out_mine_ref, out_other_ref = refs[2 + count : 4 + count]
    *store_refs, hidden_ref, rows_ref, sems = refs[4 + count :]
    half = mine_ref.shape[0]
    z, y = lax.axis_index("z"), lax.axis_index("y")
    copies = []
    which = iter(piece_refs)
    for store_ref, part in zip(store_refs, places):
        for piece in part:
            piece_ref = next(which)
            for n, (far_z, far_y) in enumerate(piece):
                shard = lax.rem(z + far_z, 8) * 4 + lax.rem(y + far_y, 4)
                copies.append(
                    pltpu.make_async_copy(piece_ref.at[n], store_ref.at[shard], sems.at[len(copies)])
                )
    for copy in copies:
        copy.start()
    rows_ref[:half] = mine_ref[...]
    rows_ref[half:] = other_ref[...]
    for copy in copies:
        copy.wait()
    tiles = [(ref, k) for ref, n in zip(store_refs, counts) for k in range(n)]
    down, gate, upper, ends = tiles[:6], tiles[6:11], tiles[11:16], tiles[16]
    for n in range(5):
        both = jnp.concatenate([flat(*gate[n]), flat(*upper[n])], axis=1)
        pair = jnp.dot(rows_ref[...], both, preferred_element_type=jnp.float32)
        hidden = pair[:, :LANES] * jax.nn.sigmoid(pair[:, :LANES]) * pair[:, LANES:]
        hidden_ref[:, n * LANES : (n + 1) * LANES] = hidden.astype(jnp.bfloat16)
    pair = jnp.dot(rows_ref[...], flat(*ends), preferred_element_type=jnp.float32)
    hidden = pair * jax.nn.sigmoid(pair) * pltpu.roll(pair, HALF, 1)
    lane = lax.broadcasted_iota(jnp.int32, hidden.shape, 1)
    hidden_ref[:, 5 * LANES :] = jnp.where(lane < HALF, hidden, 0.0).astype(jnp.bfloat16)
    for n in range(8):
        own = slice(n * 4, (n + 1) * 4)
        both = jnp.concatenate([ref[own, k].reshape(-1, LANES) for ref, k in down], axis=1)
        terms = nt_dot(hidden_ref[...], both).astype(jnp.bfloat16)
        out_mine_ref[:, n * 256 : (n + 1) * 256] = terms[:half]
        out_other_ref[:, n * 256 : (n + 1) * 256] = terms[half:]


def first_ffn_terms(rows, parts):
    half, width = rows[0].shape
    counts = tuple(part[0][0].shape[1] for part in parts)
    places = [[place for _, place in part] for part in parts]
    pieces = [piece for part in parts for piece, _ in part]
    return pl.pallas_call(
        lambda *refs: first_ffn_kernel(places, counts, *refs),
        in_specs=[pl.BlockSpec(memory_space=pltpu.VMEM)] * 2
        + [pl.BlockSpec(memory_space=pl.ANY)] * len(pieces),
        out_shape=[pltpu.VMEM((half, width), jnp.bfloat16)] * 2,
        scratch_shapes=[pltpu.VMEM((32, n, SHARD, LANES), jnp.bfloat16) for n in counts]
        + [
            pltpu.VMEM((2 * half, 6 * LANES), jnp.bfloat16),
            pltpu.VMEM((2 * half, width), jnp.bfloat16),
            pltpu.SemaphoreType.DMA((32 * len(counts),)),
        ],
        compiler_params=pltpu.CompilerParams(vmem_limit_bytes=40 << 20),
        name="first_ffn",
    )(*rows, *pieces)


def ffn_terms(rows, packed):
    shards = packed.shape[0]
    half, width = rows[0].shape
    return pl.pallas_call(
        ffn_kernel,
        grid=(6,),
        in_specs=[
            whole(half, width),
            whole(half, width),
            pl.BlockSpec((shards, 1, SHARD, LANES), lambda j: (0, jnp.where(j < 5, 6 + j, 16), 0, 0)),
            pl.BlockSpec((shards, 1, SHARD, LANES), lambda j: (0, jnp.minimum(11 + j, 15), 0, 0)),
            pl.BlockSpec((shards, 6, SHARD, LANES), lambda j: (0, 0, 0, 0)),
        ],
        out_specs=[whole(half, width)] * 2,
        out_shape=[pltpu.VMEM((half, width), jnp.bfloat16)] * 2,
        scratch_shapes=[
            pltpu.VMEM((2 * half, 6 * LANES), jnp.bfloat16),
            pltpu.VMEM((2 * half, width), jnp.bfloat16),
        ],
        compiler_params=pltpu.CompilerParams(vmem_limit_bytes=40 << 20),
        name="ffn",
    )(*rows, packed, packed, packed)


def shifted(values, by, fill):
    row = lax.broadcasted_iota(jnp.int32, values.shape, 0)
    return jnp.where(row >= by, pltpu.roll(values, by, 0), fill)


def minus_expm1(x):
    series = 1.0 + x / 8.0
    for k in range(7, 1, -1):
        series = 1.0 + (x / k) * series
    return jnp.where(x > -0.5, -x * series, 1.0 - jnp.exp(x))


def scanned(keep, drive):
    by = 1
    while by < keep.shape[0]:
        drive = keep * shifted(drive, by, 0.0) + drive
        keep = keep * shifted(keep, by, 1.0)
        by *= 2
    return drive


def mixer_kernel(
    mine_ref,
    other_ref,
    x_ref,
    gate_ref,
    ends_ref,
    out0_ref,
    out1_ref,
    taps_ref,
    a_ref,
    b_ref,
    rate_ref,
    out_mine_ref,
    out_other_ref,
    order_ref,
):
    half = mine_ref.shape[0]
    chips = lax.axis_size("x")
    block = half // chips
    x = lax.axis_index("x")
    core = lax.axis_index("c")
    weights = jnp.concatenate([flat(x_ref, 0), flat(gate_ref, 0), flat(ends_ref, 0)], axis=1)
    places = []
    for n, ref in enumerate((mine_ref, other_ref)):
        part = jnp.dot(ref[...], weights, preferred_element_type=jnp.float32)
        for k in range(chips):
            chip = lax.rem(x + k, chips)
            which = core if n == 0 else 1 - core
            place = pl.multiple_of((chip * 2 + which) * block, block)
            places.append(place)
            order_ref[pl.ds(place, block), :] = part[k * block : (k + 1) * block]
    z = order_ref[:, : 2 * LANES]
    ends = order_ref[:, 2 * LANES :]
    lane = lax.broadcasted_iota(jnp.int32, ends.shape, 1)
    groups = (
        (z[:, :LANES], z[:, LANES:]),
        (jnp.where(lane < HALF, ends, 0.0), pltpu.roll(ends, HALF, 1)),
    )
    mixed = []
    for g, (lru_x, lru_gate) in enumerate(groups):
        lru_x = lru_x.astype(jnp.bfloat16).astype(jnp.float32)
        lru_gate = lru_gate.astype(jnp.bfloat16).astype(jnp.float32)
        own = slice(g * LANES, (g + 1) * LANES)
        taps = taps_ref[:, own]
        conv = taps[0:1] * lru_x
        for k in range(1, 4):
            conv = conv + taps[k : k + 1] * shifted(lru_x, k, 0.0)
        low = conv.astype(jnp.bfloat16)
        recall = jax.nn.sigmoid(jnp.dot(low, a_ref[g], preferred_element_type=jnp.float32))
        admit = jax.nn.sigmoid(jnp.dot(low, b_ref[g], preferred_element_type=jnp.float32))
        log_keep = recall * rate_ref[:, own]
        drive = jnp.sqrt(minus_expm1(2.0 * log_keep)) * admit * low.astype(jnp.float32)
        state = scanned(jnp.exp(log_keep), drive)
        mixed.append(state * jax.nn.gelu(lru_gate))
    for g in range(2):
        order_ref[:, g * LANES : (g + 1) * LANES] = mixed[g]
    mixed = jnp.concatenate([order_ref[pl.ds(p, block), : 2 * LANES] for p in places], axis=0)
    mixed = mixed.astype(jnp.bfloat16)
    full = mixed[:, :LANES]
    short = mixed[:, LANES : LANES + HALF]
    shards = 256 // SHARD
    for n in range(out0_ref.shape[0] // shards):
        own = slice(n * shards, (n + 1) * shards)
        terms = nt_dot(full, out0_ref[own, 0].reshape(-1, LANES))
        terms = terms + nt_dot(short, out1_ref[own, 0].reshape(-1, LANES)[:, :HALF])
        terms = terms.astype(jnp.bfloat16)
        out_mine_ref[:, n * 256 : (n + 1) * 256] = terms[:half]
        out_other_ref[:, n * 256 : (n + 1) * 256] = terms[half:]


def paired_blocks(blocks):
    zero = jnp.zeros_like(blocks[0])
    top = jnp.concatenate(
        [jnp.concatenate([blocks[0], zero], 1), jnp.concatenate([zero, blocks[1]], 1)], 0
    )
    end = jnp.concatenate(
        [jnp.concatenate([blocks[2], zero], 1), jnp.concatenate([zero, zero], 1)], 0
    )
    return jnp.stack([top, end])


def mixer_terms(rows, packed, conv_weight, gate_a_weight, gate_x_weight, decay_param):
    shards = packed.shape[0]
    half, width = rows[0].shape
    pad = ((0, 0), (0, HALF))
    taps = jnp.pad(conv_weight.astype(jnp.float32), pad)
    rate = jnp.pad(-8.0 * jax.nn.softplus(-decay_param)[None], pad)
    tile = lambda k: pl.BlockSpec((shards, 1, SHARD, LANES), lambda j: (0, k, 0, 0))
    return pl.pallas_call(
        mixer_kernel,
        grid=(1,),
        in_specs=[
            whole(half, width),
            whole(half, width),
            tile(0),
            tile(1),
            tile(2),
            tile(3),
            tile(4),
            whole(4, 2 * LANES),
            whole(2, LANES, LANES),
            whole(2, LANES, LANES),
            whole(1, 2 * LANES),
        ],
        out_specs=[whole(half, width)] * 2,
        out_shape=[pltpu.VMEM((half, width), jnp.bfloat16)] * 2,
        scratch_shapes=[pltpu.VMEM((2 * half, 3 * LANES), jnp.float32)],
        compiler_params=pltpu.CompilerParams(vmem_limit_bytes=40 << 20),
        name="mixer",
    )(
        *rows,
        packed,
        packed,
        packed,
        packed,
        packed,
        taps,
        paired_blocks(gate_a_weight),
        paired_blocks(gate_x_weight),
        rate,
    )


def body(
    tokens,
    ffn1_gain,
    ffn1_gate,
    ffn1_up,
    ffn1_down,
    mix_gain,
    lru_in_weight,
    lru_gate_weight,
    conv_weight,
    gate_a_weight,
    gate_x_weight,
    decay_param,
    mix_out_weight,
    ffn2_gain,
    ffn2_gate,
    ffn2_up,
    ffn2_down,
):
    plan = full_tiles(0, 5) + [((0, 640, HALF),)]
    plan += full_tiles(1, 5) + full_tiles(2, 5) + [((1, 640, HALF), (2, 640, HALF))]
    tiles = packed_tiles(plan, [ffn1_down.T, ffn1_gate, ffn1_up], (8, 9))
    parts = [spread_z_last(tiles[0]), spread_y_last(tiles[1])]
    mixing = full_tiles(0, 1) + full_tiles(1, 1) + [((0, LANES, HALF), (1, LANES, HALF))]
    mixing += full_tiles(2, 1) + [((2, LANES, HALF),)]
    packed1 = gather_tiles(mixing, [lru_in_weight, lru_gate_weight, mix_out_weight.T])
    packed2 = gather_tiles(plan, [ffn2_down.T, ffn2_gate, ffn2_up])
    rows = gather_rows(rms_rows(tokens, ffn1_gain))
    sums = sent_sums(first_ffn_terms(rows, parts))
    first, normed = combined(tokens, sums, True, mix_gain)
    rows = gather_rows(normed)
    sums = sent_sums(
        mixer_terms(rows, packed1, conv_weight, gate_a_weight, gate_x_weight, decay_param)
    )
    second, normed = combined(first, sums, False, ffn2_gain)
    rows = gather_rows(normed)
    sums = sent_sums(ffn_terms(rows, packed2))
    return combined(second, sums, True)[0]


def solution(mesh):
    split = Mesh(mesh.devices.reshape(8, 4, 4, 2), FS_TP)
    placed = (
        P(FS_TP, None),
        P(),
        P(FS, TP),
        P(FS, TP),
        P(TP, FS),
        P(),
        P(FS, TP),
        P(FS, TP),
        P(None, TP),
        P(TP, None, None),
        P(TP, None, None),
        P(TP),
        P(TP, FS),
        P(),
        P(FS, TP),
        P(FS, TP),
        P(TP, FS),
    )
    return jax.shard_map(
        body, mesh=split, in_specs=placed, out_specs=P(FS_TP, None), check_vma=False
    )
```

```python
import jax
import jax.numpy as jnp
from jax import lax
from jax.experimental import pallas as pl
from jax.experimental.pallas import tpu as pltpu
from jax.sharding import Mesh
from jax.sharding import PartitionSpec as P

FS = ("z", "y")
TP = ("x", "c")
FS_TP = ("z", "y", "x", "c")

EPS = 1e-06
LANES = 128
SHARD = 64
HALF = 64
WIDE = 256
PARAMS = pltpu.CompilerParams(vmem_limit_bytes=24 << 20)


def moved(value, axis, by):
    count = lax.axis_size(axis)
    return lax.ppermute(value, axis, [(i, (i - by) % count) for i in range(count)])


def in_vmem(*values):
    return tuple(pltpu.with_memory_space_constraint(v, pltpu.VMEM) for v in values)


def vmem_specs(count):
    return [pl.BlockSpec(memory_space=pltpu.VMEM)] * count


def vmem_call(kernel, name, out_shape, scratch=()):
    def call(*args):
        return pl.pallas_call(
            kernel,
            in_specs=vmem_specs(len(args)),
            out_specs=jax.tree.map(lambda _: vmem_specs(1)[0], out_shape),
            out_shape=out_shape,
            scratch_shapes=list(scratch),
            compiler_params=PARAMS,
            name=name,
        )(*in_vmem(*args))

    return call


def norm_of(wide, gain):
    scale = lax.rsqrt(jnp.mean(wide * wide, axis=-1, keepdims=True) + EPS)
    return (wide * scale * gain).astype(jnp.bfloat16)


def turned_by_y(values, amount):
    groups = range(0, values.shape[1], WIDE)
    return jnp.concatenate([pltpu.roll(values[:, g : g + WIDE], amount, 1) for g in groups], axis=1)


def turned_to(values):
    z, y = lax.axis_index("z"), lax.axis_index("y")
    values = pltpu.roll(values, lax.rem(8 - z, 8) * WIDE, 1)
    return turned_by_y(values, lax.rem(4 - y, 4) * SHARD)


def turned_back(values):
    z, y = lax.axis_index("z"), lax.axis_index("y")
    return pltpu.roll(turned_by_y(values, y * SHARD), z * WIDE, 1)


def norm_kernel(rows_ref, gain_ref, out_ref):
    normed = norm_of(rows_ref[...].astype(jnp.float32), gain_ref[...])
    out_ref[...] = turned_to(normed.astype(jnp.float32)).astype(jnp.bfloat16)


def turned_norm(values, gain):
    out = pltpu.VMEM(values.shape, jnp.bfloat16)
    return vmem_call(norm_kernel, "norm", out)(values, gain[None])


def gather_rows(own):
    mine = lax.all_gather(own, "x", axis=0, tiled=True)
    return mine, moved(mine, "c", 1)


def pair_sum_kernel(mine_ref, other_ref, out_ref):
    rows = out_ref.shape[1]
    for n in range(out_ref.shape[0]):
        own = slice(n * rows, (n + 1) * rows)
        out_ref[n] = (
            mine_ref[own].astype(jnp.float32) + other_ref[own].astype(jnp.float32)
        ).astype(jnp.bfloat16)


def sent_sums(terms):
    mine, other = terms
    count = lax.axis_size("x")
    out = pltpu.VMEM((count, mine.shape[0] // count, mine.shape[1]), jnp.bfloat16)
    sums = vmem_call(pair_sum_kernel, "pair_sum", out)(mine, moved(other, "c", 1))
    return lax.all_to_all(sums, "x", split_axis=0, concat_axis=0, tiled=True)


def combine_kernel(half, turned, base_ref, sums_ref, *refs):
    total = sums_ref[0].astype(jnp.float32)
    for n in range(1, sums_ref.shape[0]):
        total = total + sums_ref[n].astype(jnp.float32)
    if turned:
        total = turned_back(total)
    if half:
        total = 0.5 * total
    result = (base_ref[...].astype(jnp.float32) + total).astype(jnp.bfloat16)
    if len(refs) == 1:
        refs[0][...] = result
    else:
        gain_ref, out_ref, norm_ref = refs
        out_ref[...] = result
        norm_ref[...] = norm_of(result.astype(jnp.float32), gain_ref[...])


def combined(base, sums, half, turned=False, gain=None):
    shape = pltpu.VMEM(base.shape, jnp.bfloat16)
    extra = () if gain is None else (gain[None],)
    outs = [shape] * (1 + len(extra))
    kernel = lambda *refs: combine_kernel(half, turned, *refs)
    return vmem_call(kernel, "combine", outs)(base, sums, *extra)


def pack_kernel(plan, out_copies, counts, *refs):
    in_refs, out_refs = refs[: -len(counts)], refs[-len(counts) :]
    places = [
        (ref, k, copies)
        for ref, count, copies in zip(out_refs, counts, out_copies)
        for k in range(count)
    ]
    for (out_ref, n, copies), parts in zip(places, plan):
        pieces = [in_refs[which][:, at : at + size] for which, at, size in parts]
        if len(pieces) == 2:
            low, high = (p.astype(jnp.float32) for p in pieces)
            tile = jnp.concatenate([low, high], axis=1).astype(jnp.bfloat16)
        else:
            tile = pieces[0]
        size = tile.shape[1]
        for at in [()] if copies == 1 else [(k,) for k in range(copies)]:
            if size < LANES:
                out_ref[(*at, n)] = jnp.zeros((SHARD, LANES), jnp.bfloat16)
            out_ref[(*at, n, slice(None), slice(0, size))] = tile


def packed_tiles(plan, arrays, counts, out_copies):
    shapes = [
        jax.ShapeDtypeStruct((*((k,) if k > 1 else ()), n, SHARD, LANES), jnp.bfloat16)
        for n, k in zip(counts, out_copies)
    ]
    return pl.pallas_call(
        lambda *refs: pack_kernel(plan, out_copies, counts, *refs), out_shape=shapes, name="pack"
    )(*arrays)


def full_tiles(which, count):
    return [((which, k * LANES, LANES),) for k in range(count)]


def spread_z_last(own):
    block = jnp.stack([own, moved(own, "y", 1), moved(own, "y", 2), moved(own, "y", 3)])
    ups, downs = [block], [block]
    for far in range(1, 4):
        ups.append(moved(ups[-1], "z", 1))
        downs.append(moved(downs[-1], "z", -1))
    across = [moved(ups[3][:2], "z", 1), moved(downs[3][2:], "z", -1)]
    return [*ups, *across, *downs[:0:-1]]


def spread_y_last(copies):
    block = lax.all_to_all(copies, "z", split_axis=0, concat_axis=0, tiled=True)
    up = moved(block, "y", 1)
    down = moved(block, "y", -1)
    cut = (block.shape[1] + 1) // 2
    return [block, up, moved(up[:, :cut], "y", 1), moved(down[:, cut:], "y", -1), down]


def nt_dot(a, b):
    return lax.dot_general(a, b, (((1,), (1,)), ((), ())), preferred_element_type=jnp.float32)


def ffn_steps(tile, down, mine_ref, other_ref, out_mine_ref, out_other_ref, hidden_ref, rows_ref):
    half = mine_ref.shape[0]
    rows_ref[:half] = mine_ref[...]
    rows_ref[half:] = other_ref[...]
    for n in range(5):
        both = jnp.concatenate([tile(n), tile(5 + n)], axis=1)
        pair = jnp.dot(rows_ref[...], both, preferred_element_type=jnp.float32)
        hidden = pair[:, :LANES] * jax.nn.sigmoid(pair[:, :LANES]) * pair[:, LANES:]
        hidden_ref[:, n * LANES : (n + 1) * LANES] = hidden.astype(jnp.bfloat16)
    pair = jnp.dot(rows_ref[...], tile(10), preferred_element_type=jnp.float32)
    hidden = pair * jax.nn.sigmoid(pair) * pltpu.roll(pair, HALF, 1)
    lane = lax.broadcasted_iota(jnp.int32, hidden.shape, 1)
    hidden_ref[:, 5 * LANES :] = jnp.where(lane < HALF, hidden, 0.0).astype(jnp.bfloat16)
    for n in range(8):
        both = jnp.concatenate([down(k, n) for k in range(6)], axis=1)
        terms = nt_dot(hidden_ref[...], both).astype(jnp.bfloat16)
        out_mine_ref[:, n * WIDE : (n + 1) * WIDE] = terms[:half]
        out_other_ref[:, n * WIDE : (n + 1) * WIDE] = terms[half:]


def first_ffn_kernel(mine_ref, other_ref, *refs):
    a_refs, b_refs = refs[:9], refs[9:14]
    z = lax.axis_index("z")
    cut = b_refs[2].shape[1]

    def block_a(k, n):
        if n == 4:
            parts = [a_refs[4][:, k], a_refs[5][:, k]]
            return jnp.concatenate(parts, axis=0).reshape(-1, LANES)
        return a_refs[n if n < 4 else n + 1][:, k].reshape(-1, LANES)

    def block_b(k, n):
        at = lax.rem(z + n, 8)
        across = b_refs[2][at, k] if k < cut else b_refs[3][at, k - cut]
        return jnp.concatenate([b_refs[0][at, k], b_refs[1][at, k], across, b_refs[4][at, k]], axis=0)

    def tile(k):
        block, which = (block_a, 6 + k) if k < 2 else (block_b, k - 2)
        return jnp.concatenate([block(which, n) for n in range(8)], axis=0)

    ffn_steps(tile, block_a, mine_ref, other_ref, *refs[14:])


def ffn_kernel(mine_ref, other_ref, packed_ref, *refs):
    def down(k, n):
        return packed_ref[n * 4 : (n + 1) * 4, 5 + k].reshape(-1, LANES)

    ffn_steps(lambda k: packed_ref[:, 11 + k].reshape(-1, LANES), down, mine_ref, other_ref, *refs)


def ffn_terms(rows, kernel, weights, name):
    half, width = rows[0].shape
    scratch = [
        pltpu.VMEM((2 * half, 6 * LANES), jnp.bfloat16),
        pltpu.VMEM((2 * half, width), jnp.bfloat16),
    ]
    outs = [pltpu.VMEM((half, width), jnp.bfloat16)] * 2
    return vmem_call(kernel, name, outs, scratch)(*rows, *weights)


def shifted(values, by, fill):
    row = lax.broadcasted_iota(jnp.int32, values.shape, 0)
    return jnp.where(row >= by, pltpu.roll(values, by, 0), fill)


def minus_expm1(x):
    series = 1.0 + x / 8.0
    for k in range(7, 1, -1):
        series = 1.0 + (x / k) * series
    return jnp.where(x > -0.5, -x * series, 1.0 - jnp.exp(x))


def scanned(keep, drive):
    by = 1
    while by < keep.shape[0]:
        drive = keep * shifted(drive, by, 0.0) + drive
        keep = keep * shifted(keep, by, 1.0)
        by *= 2
    return drive


def mixer_kernel(
    mine_ref, other_ref, packed_ref, taps_ref, a_ref, b_ref, rate_ref, out_mine_ref, out_other_ref, order_ref
):
    half = mine_ref.shape[0]
    chips = lax.axis_size("x")
    block = half // chips
    core = lax.axis_index("c")
    weights = jnp.concatenate([packed_ref[:, k].reshape(-1, LANES) for k in range(3)], axis=1)
    places = []
    for n, ref in enumerate((mine_ref, other_ref)):
        part = jnp.dot(ref[...], weights, preferred_element_type=jnp.float32)
        which = core if n == 0 else 1 - core
        for chip in range(chips):
            place = pl.multiple_of((chip * 2 + which) * block, block)
            places.append(place)
            order_ref[pl.ds(place, block), :] = part[chip * block : (chip + 1) * block]
    z = order_ref[:, : 2 * LANES]
    ends = order_ref[:, 2 * LANES :]
    lane = lax.broadcasted_iota(jnp.int32, ends.shape, 1)
    groups = (
        (z[:, :LANES], z[:, LANES:]),
        (jnp.where(lane < HALF, ends, 0.0), pltpu.roll(ends, HALF, 1)),
    )
    mixed = []
    for g, (lru_x, lru_gate) in enumerate(groups):
        lru_x = lru_x.astype(jnp.bfloat16).astype(jnp.float32)
        lru_gate = lru_gate.astype(jnp.bfloat16).astype(jnp.float32)
        own = slice(g * LANES, (g + 1) * LANES)
        taps = taps_ref[:, own]
        conv = taps[0:1] * lru_x
        for k in range(1, 4):
            conv = conv + taps[k : k + 1] * shifted(lru_x, k, 0.0)
        low = conv.astype(jnp.bfloat16)
        recall = jax.nn.sigmoid(jnp.dot(low, a_ref[g], preferred_element_type=jnp.float32))
        admit = jax.nn.sigmoid(jnp.dot(low, b_ref[g], preferred_element_type=jnp.float32))
        log_keep = recall * rate_ref[:, own]
        drive = jnp.sqrt(minus_expm1(2.0 * log_keep)) * admit * low.astype(jnp.float32)
        state = scanned(jnp.exp(log_keep), drive)
        mixed.append(state * jax.nn.gelu(lru_gate))
    for g in range(2):
        order_ref[:, g * LANES : (g + 1) * LANES] = mixed[g]
    mixed = jnp.concatenate([order_ref[pl.ds(p, block), : 2 * LANES] for p in places], axis=0)
    mixed = mixed.astype(jnp.bfloat16)
    full = mixed[:, :LANES]
    short = mixed[:, LANES : LANES + HALF]
    for n in range(8):
        own = slice(n * 4, (n + 1) * 4)
        terms = nt_dot(full, packed_ref[own, 3].reshape(-1, LANES))
        terms = terms + nt_dot(short, packed_ref[own, 4].reshape(-1, LANES)[:, :HALF])
        terms = terms.astype(jnp.bfloat16)
        out_mine_ref[:, n * WIDE : (n + 1) * WIDE] = terms[:half]
        out_other_ref[:, n * WIDE : (n + 1) * WIDE] = terms[half:]


def paired_blocks(blocks):
    zero = jnp.zeros_like(blocks[0])
    top = jnp.concatenate(
        [jnp.concatenate([blocks[0], zero], 1), jnp.concatenate([zero, blocks[1]], 1)], 0
    )
    end = jnp.concatenate(
        [jnp.concatenate([blocks[2], zero], 1), jnp.concatenate([zero, zero], 1)], 0
    )
    return jnp.stack([top, end])


def mixer_terms(rows, packed, conv_weight, gate_a_weight, gate_x_weight, decay_param):
    half, width = rows[0].shape
    pad = ((0, 0), (0, HALF))
    taps = jnp.pad(conv_weight.astype(jnp.float32), pad)
    rate = jnp.pad(-8.0 * jax.nn.softplus(-decay_param)[None], pad)
    outs = [pltpu.VMEM((half, width), jnp.bfloat16)] * 2
    scratch = [pltpu.VMEM((2 * half, 3 * LANES), jnp.float32)]
    return vmem_call(mixer_kernel, "mixer", outs, scratch)(
        *rows, packed, taps, paired_blocks(gate_a_weight), paired_blocks(gate_x_weight), rate
    )


def body(
    tokens,
    ffn1_gain,
    ffn1_gate,
    ffn1_up,
    ffn1_down,
    mix_gain,
    lru_in_weight,
    lru_gate_weight,
    conv_weight,
    gate_a_weight,
    gate_x_weight,
    decay_param,
    mix_out_weight,
    ffn2_gain,
    ffn2_gate,
    ffn2_up,
    ffn2_down,
):
    ends = [((1, 640, HALF), (2, 640, HALF))]
    gates, uppers = full_tiles(1, 5), full_tiles(2, 5)
    downs = full_tiles(0, 5) + [((0, 640, HALF),)]
    order = gates + uppers + ends
    plan = downs + order
    own, copies = packed_tiles(plan, [ffn1_down.T, ffn1_gate, ffn1_up], (8, 9), (1, 8))
    weights = spread_z_last(own) + spread_y_last(copies)

    mixing = full_tiles(3, 1) + full_tiles(4, 1) + [((3, LANES, HALF), (4, LANES, HALF))]
    mixing += full_tiles(5, 1) + [((5, LANES, HALF),)]
    plan = mixing + downs + order
    (packed,) = packed_tiles(
        plan,
        [ffn2_down.T, ffn2_gate, ffn2_up, lru_in_weight, lru_gate_weight, mix_out_weight.T],
        (len(plan),),
        (1,),
    )
    packed = lax.all_gather(packed.reshape(-1, LANES), FS, axis=0, tiled=True)
    packed = packed.reshape(-1, len(plan), SHARD, LANES)

    normed = turned_norm(tokens, ffn1_gain)
    normed, _ = lax.optimization_barrier((normed, weights[1]))
    rows = gather_rows(normed)
    sums = sent_sums(ffn_terms(rows, first_ffn_kernel, weights, "first_ffn"))
    first, normed = combined(tokens, sums, True, True, mix_gain)
    rows = gather_rows(normed)
    sums = sent_sums(
        mixer_terms(rows, packed, conv_weight, gate_a_weight, gate_x_weight, decay_param)
    )
    second, normed = combined(first, sums, False, False, ffn2_gain)
    rows = gather_rows(normed)
    sums = sent_sums(ffn_terms(rows, ffn_kernel, [packed], "ffn"))
    return combined(second, sums, True)[0]


def solution(mesh):
    split = Mesh(mesh.devices.reshape(8, 4, 4, 2), FS_TP)
    placed = (
        P(FS_TP, None),
        P(),
        P(FS, TP),
        P(FS, TP),
        P(TP, FS),
        P(),
        P(FS, TP),
        P(FS, TP),
        P(None, TP),
        P(TP, None, None),
        P(TP, None, None),
        P(TP),
        P(TP, FS),
        P(),
        P(FS, TP),
        P(FS, TP),
        P(TP, FS),
    )
    return jax.shard_map(
        body, mesh=split, in_specs=placed, out_specs=P(FS_TP, None), check_vma=False
    )
```

```python
import jax
import jax.numpy as jnp
from jax import lax
from jax.experimental import pallas as pl
from jax.experimental.pallas import tpu as pltpu
from jax.sharding import Mesh
from jax.sharding import PartitionSpec as P

FS = ("z", "y")
TP = ("x", "c")
FS_TP = ("z", "y", "x", "c")

EPS = 1e-06
LANES = 128
SHARD = 64
HALF = 64
WIDE = 256
FFN_LOOPED = (False, True)
PARAMS = pltpu.CompilerParams(vmem_limit_bytes=24 << 20)


def moved(value, axis, by):
    count = lax.axis_size(axis)
    return lax.ppermute(value, axis, [(i, (i - by) % count) for i in range(count)])


def in_vmem(*values):
    return tuple(pltpu.with_memory_space_constraint(v, pltpu.VMEM) for v in values)


def vmem_specs(count):
    return [pl.BlockSpec(memory_space=pltpu.VMEM)] * count


def vmem_call(kernel, out_shape, scratch=()):
    def call(*args):
        return pl.pallas_call(
            kernel,
            in_specs=vmem_specs(len(args)),
            out_specs=jax.tree.map(lambda _: vmem_specs(1)[0], out_shape),
            out_shape=out_shape,
            scratch_shapes=list(scratch),
            compiler_params=PARAMS,
        )(*in_vmem(*args))

    return call


def norm_of(wide, gain):
    scale = lax.rsqrt(jnp.mean(wide * wide, axis=-1, keepdims=True) + EPS)
    return (wide * scale * gain).astype(jnp.bfloat16)


def turned_by_y(values, amount):
    groups = range(0, values.shape[1], WIDE)
    return jnp.concatenate([pltpu.roll(values[:, g : g + WIDE], amount, 1) for g in groups], axis=1)


def turned_to(values, axes):
    z, y = lax.axis_index("z"), lax.axis_index("y")
    if "z" in axes:
        values = pltpu.roll(values, lax.rem(8 - z, 8) * WIDE, 1)
    if "y" in axes:
        values = turned_by_y(values, lax.rem(4 - y, 4) * SHARD)
    return values


def turned_back(values, axes):
    z, y = lax.axis_index("z"), lax.axis_index("y")
    if "y" in axes:
        values = turned_by_y(values, y * SHARD)
    if "z" in axes:
        values = pltpu.roll(values, z * WIDE, 1)
    return values


def turned_norm_of(wide, gain, axes):
    normed = norm_of(wide, gain)
    if axes:
        normed = turned_to(normed.astype(jnp.float32), axes).astype(jnp.bfloat16)
    return normed


def norm_kernel(rows_ref, gain_ref, out_ref):
    out_ref[...] = turned_norm_of(rows_ref[...].astype(jnp.float32), gain_ref[...], "zy")


def turned_norm(values, gain):
    out = pltpu.VMEM(values.shape, jnp.bfloat16)
    return vmem_call(norm_kernel, out)(values, gain[None])


def gather_rows(own):
    mine = lax.all_gather(own, "x", axis=0, tiled=True)
    return mine, moved(mine, "c", 1)


def pair_sum_kernel(mine_ref, other_ref, out_ref):
    rows = out_ref.shape[1]
    for n in range(out_ref.shape[0]):
        own = slice(n * rows, (n + 1) * rows)
        out_ref[n] = (
            mine_ref[own].astype(jnp.float32) + other_ref[own].astype(jnp.float32)
        ).astype(jnp.bfloat16)


def sent_sums(terms):
    mine, other = terms
    count = lax.axis_size("x")
    out = pltpu.VMEM((count, mine.shape[0] // count, mine.shape[1]), jnp.bfloat16)
    other = moved(other, "c", 1)
    sums = vmem_call(pair_sum_kernel, out)(mine, other)
    return lax.all_to_all(sums, "x", split_axis=0, concat_axis=0, tiled=True)


def combine_kernel(half, turned, turn, base_ref, sums_ref, *refs):
    total = sums_ref[0].astype(jnp.float32)
    for n in range(1, sums_ref.shape[0]):
        total = total + sums_ref[n].astype(jnp.float32)
    total = turned_back(total, turned)
    if half:
        total = 0.5 * total
    result = (base_ref[...].astype(jnp.float32) + total).astype(jnp.bfloat16)
    if len(refs) == 1:
        refs[0][...] = result
    else:
        gain_ref, out_ref, norm_ref = refs
        out_ref[...] = result
        norm_ref[...] = turned_norm_of(result.astype(jnp.float32), gain_ref[...], turn)


def combined(base, sums, half, turned="", gain=None, turn=""):
    shape = pltpu.VMEM(base.shape, jnp.bfloat16)
    extra = () if gain is None else (gain[None],)
    outs = [shape] * 2 if extra else [jax.ShapeDtypeStruct(base.shape, jnp.bfloat16)]
    kernel = lambda *refs: combine_kernel(half, turned, turn, *refs)
    return vmem_call(kernel, outs)(base, sums, *extra)


def pack_kernel(plan, out_copies, counts, *refs):
    in_refs, out_refs = refs[: -len(counts)], refs[-len(counts) :]
    places = [
        (ref, k, copies)
        for ref, count, copies in zip(out_refs, counts, out_copies)
        for k in range(count)
    ]
    for (out_ref, n, copies), parts in zip(places, plan):
        pieces = [in_refs[which][:, at : at + size] for which, at, size in parts]
        if len(pieces) == 2:
            low, high = (p.astype(jnp.float32) for p in pieces)
            tile = jnp.concatenate([low, high], axis=1).astype(jnp.bfloat16)
        else:
            tile = pieces[0]
        size = tile.shape[1]
        for at in [()] if copies == 1 else [(k,) for k in range(copies)]:
            if size < LANES:
                out_ref[(*at, n)] = jnp.zeros((SHARD, LANES), jnp.bfloat16)
            out_ref[(*at, n, slice(None), slice(0, size))] = tile


def packed_tiles(plan, arrays, counts, out_copies):
    shapes = [
        jax.ShapeDtypeStruct((*((k,) if k > 1 else ()), n, SHARD, LANES), jnp.bfloat16)
        for n, k in zip(counts, out_copies)
    ]
    return pl.pallas_call(
        lambda *refs: pack_kernel(plan, out_copies, counts, *refs),
        out_shape=shapes,
        compiler_params=PARAMS,
        name="pack",
    )(*[in_hbm(a) for a in arrays])


def gather_tiles(plan, arrays):
    (packed,) = packed_tiles(plan, arrays, (len(plan),), (1,))
    full = lax.all_gather(packed.reshape(-1, LANES), FS, axis=0, tiled=True)
    return full.reshape(-1, len(plan), SHARD, LANES)


def full_tiles(which, count):
    return [((which, k * LANES, LANES),) for k in range(count)]


def after(value, *others):
    return lax.optimization_barrier((value, *others))[0]


def in_hbm(value):
    return pltpu.with_memory_space_constraint(value, pltpu.HBM)


def both_ways(up, down, axis):
    return lax.optimization_barrier((moved(up, axis, 1), moved(down, axis, -1)))


def spread_z_last(block, *others):
    up = down = after(block, *others)
    ups, downs = [block], []
    for _ in range(1, 4):
        up, down = both_ways(up, down, "z")
        ups.append(up)
        downs.insert(0, down)
    return [*ups, moved(up, "z", 1), *downs]


def join_kernel(*refs):
    *part_refs, out_ref = refs
    for n, ref in enumerate(part_refs):
        out_ref[n] = ref[...]


def spread_over_z(own):
    up = down = own
    ups, downs = [own], []
    for _ in range(1, 4):
        up, down = both_ways(up, down, "z")
        ups.append(up)
        downs.insert(0, down)
    parts = [*ups, moved(up, "z", 1), *downs]
    out = pltpu.VMEM((8, *own.shape), jnp.bfloat16)
    return vmem_call(join_kernel, out)(*parts), up, down


def spread_over_y(block):
    up, down = both_ways(block, block, "y")
    cut = (block.shape[1] + 1) // 2
    across = [moved(up[:, :cut], "y", 1), moved(down[:, cut:], "y", -1)]
    return [block, up, *across, down]


def nt_dot(a, b):
    return lax.dot_general(a, b, (((1,), (1,)), ((), ())), preferred_element_type=jnp.float32)


def steps(count, step, looped):
    if looped:
        lax.fori_loop(0, count, lambda n, carry: (step(n), carry)[1], 0)
    else:
        for n in range(count):
            step(n)


def lanes(n, size):
    return pl.ds(n * size if isinstance(n, int) else pl.multiple_of(n * size, size), size)


def ffn_steps(looped, tile, down, mine_ref, other_ref, out_mine_ref, out_other_ref, hidden_ref, rows_ref):
    half = mine_ref.shape[0]
    rows_ref[:half] = mine_ref[...]
    rows_ref[half:] = other_ref[...]

    def hidden_step(n):
        both = jnp.concatenate([tile(n), tile(5 + n)], axis=1)
        pair = jnp.dot(rows_ref[...], both, preferred_element_type=jnp.float32)
        hidden = pair[:, :LANES] * jax.nn.sigmoid(pair[:, :LANES]) * pair[:, LANES:]
        hidden_ref[:, lanes(n, LANES)] = hidden.astype(jnp.bfloat16)

    steps(5, hidden_step, looped[0])
    pair = jnp.dot(rows_ref[...], tile(10), preferred_element_type=jnp.float32)
    hidden = pair * jax.nn.sigmoid(pair) * pltpu.roll(pair, HALF, 1)
    lane = lax.broadcasted_iota(jnp.int32, hidden.shape, 1)
    hidden_ref[:, 5 * LANES :] = jnp.where(lane < HALF, hidden, 0.0).astype(jnp.bfloat16)

    def down_step(n):
        both = jnp.concatenate([down(k, n) for k in range(6)], axis=1)
        terms = nt_dot(hidden_ref[...], both).astype(jnp.bfloat16)
        out_mine_ref[:, lanes(n, WIDE)] = terms[:half]
        out_other_ref[:, lanes(n, WIDE)] = terms[half:]

    steps(8, down_step, looped[1])


def first_ffn_kernel(mine_ref, other_ref, *refs):
    a_refs, b_refs = refs[:8], refs[8:13]
    y = lax.axis_index("y")
    cut = b_refs[2].shape[1]

    def block_a(k, n):
        return jnp.concatenate([a_refs[n][lax.rem(y + q, 4), k] for q in range(4)], axis=0)

    def block_b(k, n):
        across = b_refs[2][n, k] if k < cut else b_refs[3][n, k - cut]
        return jnp.concatenate([b_refs[0][n, k], b_refs[1][n, k], across, b_refs[4][n, k]], axis=0)

    def tile(k):
        block, which = (block_a, 6 + k) if k < 2 else (block_b, k - 2)
        return jnp.concatenate([block(which, n) for n in range(8)], axis=0)

    ffn_steps((False, False), tile, block_a, mine_ref, other_ref, *refs[13:])


def ffn_kernel(mine_ref, other_ref, packed_ref, *refs):
    def down(k, n):
        return packed_ref[pl.ds(n * 4, 4), k].reshape(-1, LANES)

    ffn_steps(FFN_LOOPED, lambda k: packed_ref[:, 6 + k].reshape(-1, LANES), down, mine_ref, other_ref, *refs)


def ffn_terms(rows, kernel, weights):
    half, width = rows[0].shape
    scratch = [
        pltpu.VMEM((2 * half, 6 * LANES), jnp.bfloat16),
        pltpu.VMEM((2 * half, width), jnp.bfloat16),
    ]
    outs = [pltpu.VMEM((half, width), jnp.bfloat16)] * 2
    return vmem_call(kernel, outs, scratch)(*rows, *weights)


def shifted(values, by, fill):
    row = lax.broadcasted_iota(jnp.int32, values.shape, 0)
    return jnp.where(row >= by, pltpu.roll(values, by, 0), fill)


def minus_expm1(x):
    series = 1.0 + x / 8.0
    for k in range(7, 1, -1):
        series = 1.0 + (x / k) * series
    return jnp.where(x > -0.5, -x * series, 1.0 - jnp.exp(x))


def scanned(keep, drive):
    by = 1
    while by < keep.shape[0]:
        drive = keep * shifted(drive, by, 0.0) + drive
        keep = keep * shifted(keep, by, 1.0)
        by *= 2
    return drive


def mixer_kernel(
    mine_ref, other_ref, packed_ref, taps_ref, a_ref, b_ref, rate_ref, out_mine_ref, out_other_ref, order_ref
):
    half = mine_ref.shape[0]
    chips = lax.axis_size("x")
    block = half // chips
    core = lax.axis_index("c")


    def tile(k, n):
        return packed_ref[pl.ds(n * 4, 4), k].reshape(-1, LANES)

    weights = [jnp.concatenate([tile(k, n) for n in range(8)], axis=0) for k in range(3)]
    weights = jnp.concatenate(weights, axis=1)
    places = []
    for n, ref in enumerate((mine_ref, other_ref)):
        part = jnp.dot(ref[...], weights, preferred_element_type=jnp.float32)
        which = core if n == 0 else 1 - core
        for chip in range(chips):
            place = pl.multiple_of((chip * 2 + which) * block, block)
            places.append(place)
            order_ref[pl.ds(place, block), :] = part[chip * block : (chip + 1) * block]
    z = order_ref[:, : 2 * LANES]
    ends = order_ref[:, 2 * LANES :]
    lane = lax.broadcasted_iota(jnp.int32, ends.shape, 1)
    groups = (
        (z[:, :LANES], z[:, LANES:]),
        (jnp.where(lane < HALF, ends, 0.0), pltpu.roll(ends, HALF, 1)),
    )
    mixed = []
    for g, (lru_x, lru_gate) in enumerate(groups):
        lru_x = lru_x.astype(jnp.bfloat16).astype(jnp.float32)
        lru_gate = lru_gate.astype(jnp.bfloat16).astype(jnp.float32)
        own = slice(g * LANES, (g + 1) * LANES)
        taps = taps_ref[:, own]
        conv = taps[0:1] * lru_x
        for k in range(1, 4):
            conv = conv + taps[k : k + 1] * shifted(lru_x, k, 0.0)
        low = conv.astype(jnp.bfloat16)
        recall = jax.nn.sigmoid(jnp.dot(low, a_ref[g], preferred_element_type=jnp.float32))
        admit = jax.nn.sigmoid(jnp.dot(low, b_ref[g], preferred_element_type=jnp.float32))
        log_keep = recall * rate_ref[:, own]
        drive = jnp.sqrt(minus_expm1(2.0 * log_keep)) * admit * low.astype(jnp.float32)
        state = scanned(jnp.exp(log_keep), drive)
        mixed.append(state * jax.nn.gelu(lru_gate))
    for g in range(2):
        order_ref[:, g * LANES : (g + 1) * LANES] = mixed[g]
    mixed = jnp.concatenate([order_ref[pl.ds(p, block), : 2 * LANES] for p in places], axis=0)
    mixed = mixed.astype(jnp.bfloat16)
    full = mixed[:, :LANES]
    short = mixed[:, LANES : LANES + HALF]

    def out_step(n):
        terms = nt_dot(full, tile(3, n)) + nt_dot(short, tile(4, n)[:, :HALF])
        terms = terms.astype(jnp.bfloat16)
        out_mine_ref[:, lanes(n, WIDE)] = terms[:half]
        out_other_ref[:, lanes(n, WIDE)] = terms[half:]

    steps(8, out_step, True)


def paired_blocks(blocks):
    zero = jnp.zeros_like(blocks[0])
    top = jnp.concatenate(
        [jnp.concatenate([blocks[0], zero], 1), jnp.concatenate([zero, blocks[1]], 1)], 0
    )
    end = jnp.concatenate(
        [jnp.concatenate([blocks[2], zero], 1), jnp.concatenate([zero, zero], 1)], 0
    )
    return jnp.stack([top, end])


def mixer_terms(rows, packed, conv_weight, gate_a_weight, gate_x_weight, decay_param):
    half, width = rows[0].shape
    pad = ((0, 0), (0, HALF))
    taps = jnp.pad(conv_weight.astype(jnp.float32), pad)
    rate = jnp.pad(-8.0 * jax.nn.softplus(-decay_param)[None], pad)
    outs = [pltpu.VMEM((half, width), jnp.bfloat16)] * 2
    scratch = [pltpu.VMEM((2 * half, 3 * LANES), jnp.float32)]
    return vmem_call(mixer_kernel, outs, scratch)(
        *rows, packed, taps, paired_blocks(gate_a_weight), paired_blocks(gate_x_weight), rate
    )


def body(
    tokens,
    ffn1_gain,
    ffn1_gate,
    ffn1_up,
    ffn1_down,
    mix_gain,
    lru_in_weight,
    lru_gate_weight,
    conv_weight,
    gate_a_weight,
    gate_x_weight,
    decay_param,
    mix_out_weight,
    ffn2_gain,
    ffn2_gate,
    ffn2_up,
    ffn2_down,
):
    ends = [((1, 640, HALF), (2, 640, HALF))]
    gates, uppers = full_tiles(1, 5), full_tiles(2, 5)
    downs = full_tiles(0, 5) + [((0, 640, HALF),)]
    order = gates + uppers + ends
    mixing = full_tiles(0, 1) + full_tiles(1, 1) + [((0, LANES, HALF), (1, LANES, HALF))]
    mixing += full_tiles(2, 1) + [((2, LANES, HALF),)]
    packed_mixing = gather_tiles(
        mixing, [lru_in_weight, lru_gate_weight, mix_out_weight.T]
    )
    packed = gather_tiles(downs + order, [ffn2_down.T, ffn2_gate, ffn2_up])

    own, others = packed_tiles(downs + order, [ffn1_down.T, ffn1_gate, ffn1_up], (8, 9), (1, 1))
    own = lax.all_gather(own, "y", axis=0)
    block, *far = spread_over_z(others)
    weights = spread_z_last(own, *far) + spread_over_y(block)

    normed = turned_norm(tokens, ffn1_gain)
    normed = after(normed, block)
    rows = gather_rows(normed)
    sums = sent_sums(ffn_terms(rows, first_ffn_kernel, weights))
    first, normed = combined(tokens, sums, True, "zy", mix_gain)
    rows = gather_rows(normed)
    sums = sent_sums(
        mixer_terms(rows, packed_mixing, conv_weight, gate_a_weight, gate_x_weight, decay_param),
    )
    second, normed = combined(first, sums, False, "", ffn2_gain)
    rows = gather_rows(normed)
    sums = sent_sums(ffn_terms(rows, ffn_kernel, [packed]))
    return combined(second, sums, True)[0]


def solution(mesh):
    split = Mesh(mesh.devices.reshape(8, 4, 4, 2), FS_TP)
    placed = (
        P(FS_TP, None),
        P(),
        P(FS, TP),
        P(FS, TP),
        P(TP, FS),
        P(),
        P(FS, TP),
        P(FS, TP),
        P(None, TP),
        P(TP, None, None),
        P(TP, None, None),
        P(TP),
        P(TP, FS),
        P(),
        P(FS, TP),
        P(FS, TP),
        P(TP, FS),
    )

    return jax.shard_map(
        body, mesh=split, in_specs=placed, out_specs=P(FS_TP, None), check_vma=False
    )
```

```python
import jax
import jax.numpy as jnp
from jax import lax
from jax.experimental import pallas as pl
from jax.experimental.pallas import tpu as pltpu
from jax.sharding import Mesh
from jax.sharding import PartitionSpec as P

FS = ("z", "y")
TP = ("x", "c")
FS_TP = ("z", "y", "x", "c")

EPS = 1e-06
LANES = 128
SHARD = 64
HALF = 64
WIDE = 256
FFN_LOOPED = (False, False)
PARAMS = pltpu.CompilerParams(vmem_limit_bytes=24 << 20)


def moved(value, axis, by):
    count = lax.axis_size(axis)
    return lax.ppermute(value, axis, [(i, (i - by) % count) for i in range(count)])


def in_vmem(*values):
    return tuple(pltpu.with_memory_space_constraint(v, pltpu.VMEM) for v in values)


def vmem_specs(count):
    return [pl.BlockSpec(memory_space=pltpu.VMEM)] * count


def vmem_call(kernel, out_shape, scratch=()):
    def call(*args):
        return pl.pallas_call(
            kernel,
            in_specs=vmem_specs(len(args)),
            out_specs=jax.tree.map(lambda _: vmem_specs(1)[0], out_shape),
            out_shape=out_shape,
            scratch_shapes=list(scratch),
            compiler_params=PARAMS,
        )(*in_vmem(*args))

    return call


def norm_of(wide, gain):
    scale = lax.rsqrt(jnp.mean(wide * wide, axis=-1, keepdims=True) + EPS)
    return (wide * scale * gain).astype(jnp.bfloat16)


def turned_by_y(values, amount):
    groups = range(0, values.shape[1], WIDE)
    return jnp.concatenate([pltpu.roll(values[:, g : g + WIDE], amount, 1) for g in groups], axis=1)


def turned_to(values, axes):
    z, y = lax.axis_index("z"), lax.axis_index("y")
    if "z" in axes:
        values = pltpu.roll(values, lax.rem(8 - z, 8) * WIDE, 1)
    if "y" in axes:
        values = turned_by_y(values, lax.rem(4 - y, 4) * SHARD)
    return values


def turned_back(values, axes):
    z, y = lax.axis_index("z"), lax.axis_index("y")
    if "y" in axes:
        values = turned_by_y(values, y * SHARD)
    if "z" in axes:
        values = pltpu.roll(values, z * WIDE, 1)
    return values


def turned_norm_of(wide, gain, axes):
    normed = norm_of(wide, gain)
    if axes:
        normed = turned_to(normed.astype(jnp.float32), axes).astype(jnp.bfloat16)
    return normed


def norm_kernel(rows_ref, gain_ref, out_ref):
    out_ref[...] = turned_norm_of(rows_ref[...].astype(jnp.float32), gain_ref[...], "zy")


def turned_norm(values, gain):
    out = pltpu.VMEM(values.shape, jnp.bfloat16)
    return vmem_call(norm_kernel, out)(values, gain[None])


def gather_rows(own):
    mine = lax.all_gather(own, "x", axis=0, tiled=True)
    return mine, moved(mine, "c", 1)


def pair_sum_kernel(mine_ref, other_ref, out_ref):
    rows = out_ref.shape[1]
    for n in range(out_ref.shape[0]):
        own = slice(n * rows, (n + 1) * rows)
        out_ref[n] = (
            mine_ref[own].astype(jnp.float32) + other_ref[own].astype(jnp.float32)
        ).astype(jnp.bfloat16)


def sent_sums(terms):
    mine, other = terms
    count = lax.axis_size("x")
    out = pltpu.VMEM((count, mine.shape[0] // count, mine.shape[1]), jnp.bfloat16)
    other = moved(other, "c", 1)
    sums = vmem_call(pair_sum_kernel, out)(mine, other)
    return [lax.all_to_all(sums, "x", split_axis=0, concat_axis=0, tiled=True)]


def apart_kernel(mine_ref, other_ref, *out_refs):
    rows, chips = out_refs[0].shape[0], len(out_refs)
    for n, out_ref in enumerate(out_refs):
        chip = lax.rem(lax.axis_index("x") + n, chips)
        own = pl.ds(pl.multiple_of(chip * rows, rows), rows)
        out_ref[...] = (
            mine_ref[own].astype(jnp.float32) + other_ref[own].astype(jnp.float32)
        ).astype(jnp.bfloat16)


def last_sums(terms):
    mine, other = terms
    count = lax.axis_size("x")
    outs = [pltpu.VMEM((mine.shape[0] // count, mine.shape[1]), jnp.bfloat16)] * count
    sums = vmem_call(apart_kernel, outs)(mine, moved(other, "c", 1))
    return [sums[0]] + [moved(sums[n], "x", -n) for n in range(1, count)]


def combine_kernel(half, turned, turn, parts, base_ref, *refs):
    sums, refs = refs[:parts], refs[parts:]
    if parts == 1:
        sums = [sums[0].at[n] for n in range(sums[0].shape[0])]
    total = sums[0][...].astype(jnp.float32)
    for part_ref in sums[1:]:
        total = total + part_ref[...].astype(jnp.float32)
    total = turned_back(total, turned)
    if half:
        total = 0.5 * total
    result = (base_ref[...].astype(jnp.float32) + total).astype(jnp.bfloat16)
    if len(refs) == 1:
        refs[0][...] = result
    else:
        gain_ref, out_ref, norm_ref = refs
        out_ref[...] = result
        norm_ref[...] = turned_norm_of(result.astype(jnp.float32), gain_ref[...], turn)


def combined(base, sums, half, turned="", gain=None, turn=""):
    shape = pltpu.VMEM(base.shape, jnp.bfloat16)
    extra = () if gain is None else (gain[None],)
    outs = [shape] * 2 if extra else [jax.ShapeDtypeStruct(base.shape, jnp.bfloat16)]
    kernel = lambda *refs: combine_kernel(half, turned, turn, len(sums), *refs)
    return vmem_call(kernel, outs)(base, *sums, *extra)


def pack_kernel(plan, out_copies, counts, *refs):
    in_refs, out_refs = refs[: -len(counts)], refs[-len(counts) :]
    places = [
        (ref, k, copies)
        for ref, count, copies in zip(out_refs, counts, out_copies)
        for k in range(count)
    ]
    for (out_ref, n, copies), parts in zip(places, plan):
        pieces = [in_refs[which][:, at : at + size] for which, at, size in parts]
        if len(pieces) == 2:
            low, high = (p.astype(jnp.float32) for p in pieces)
            tile = jnp.concatenate([low, high], axis=1).astype(jnp.bfloat16)
        else:
            tile = pieces[0]
        size = tile.shape[1]
        for at in [()] if copies == 1 else [(k,) for k in range(copies)]:
            if size < LANES:
                out_ref[(*at, n)] = jnp.zeros((SHARD, LANES), jnp.bfloat16)
            out_ref[(*at, n, slice(None), slice(0, size))] = tile


def packed_tiles(plan, arrays, counts, out_copies):
    shapes = [
        jax.ShapeDtypeStruct((*((k,) if k > 1 else ()), n, SHARD, LANES), jnp.bfloat16)
        for n, k in zip(counts, out_copies)
    ]
    return pl.pallas_call(
        lambda *refs: pack_kernel(plan, out_copies, counts, *refs),
        out_shape=shapes,
        compiler_params=PARAMS,
        name="pack",
    )(*[in_hbm(a) for a in arrays])


def gather_tiles(packed):
    full = lax.all_gather(packed.reshape(-1, LANES), FS, axis=0, tiled=True)
    return full.reshape(-1, *packed.shape)


def full_tiles(which, count):
    return [((which, k * LANES, LANES),) for k in range(count)]


def after(value, *others):
    return lax.optimization_barrier((value, *others))[0]


def in_hbm(value):
    return pltpu.with_memory_space_constraint(value, pltpu.HBM)


def both_ways(up, down, axis):
    return lax.optimization_barrier((moved(up, axis, 1), moved(down, axis, -1)))


def spread_z_last(block, *others):
    up = down = after(block, *others)
    ups, downs = [block], []
    for _ in range(1, 4):
        up, down = both_ways(up, down, "z")
        ups.append(up)
        downs.insert(0, down)
    return [*ups, moved(up, "z", 1), *downs]


def join_kernel(*refs):
    *part_refs, out_ref = refs
    for n, ref in enumerate(part_refs):
        out_ref[n] = ref[...]


def spread_over_z(own):
    up = down = own
    ups, downs = [own], []
    for _ in range(1, 4):
        up, down = both_ways(up, down, "z")
        ups.append(up)
        downs.insert(0, down)
    parts = [*ups, moved(up, "z", 1), *downs]
    out = pltpu.VMEM((8, *own.shape), jnp.bfloat16)
    return vmem_call(join_kernel, out)(*parts), up, down


def spread_over_y(block):
    up, down = both_ways(block, block, "y")
    cut = (block.shape[1] + 1) // 2
    across = [moved(up[:, :cut], "y", 1), moved(down[:, cut:], "y", -1)]
    return [block, up, *across, down]


def nt_dot(a, b):
    return lax.dot_general(a, b, (((1,), (1,)), ((), ())), preferred_element_type=jnp.float32)


def steps(count, step, looped):
    if looped:
        lax.fori_loop(0, count, lambda n, carry: (step(n), carry)[1], 0)
    else:
        for n in range(count):
            step(n)


def lanes(n, size):
    return pl.ds(n * size if isinstance(n, int) else pl.multiple_of(n * size, size), size)


def ffn_steps(looped, tile, down, mine_ref, other_ref, out_mine_ref, out_other_ref, hidden_ref, rows_ref):
    half = mine_ref.shape[0]
    rows_ref[:half] = mine_ref[...]
    rows_ref[half:] = other_ref[...]

    def hidden_step(n):
        both = jnp.concatenate([tile(n), tile(5 + n)], axis=1)
        pair = jnp.dot(rows_ref[...], both, preferred_element_type=jnp.float32)
        hidden = pair[:, :LANES] * jax.nn.sigmoid(pair[:, :LANES]) * pair[:, LANES:]
        hidden_ref[:, lanes(n, LANES)] = hidden.astype(jnp.bfloat16)

    steps(5, hidden_step, looped[0])
    pair = jnp.dot(rows_ref[...], tile(10), preferred_element_type=jnp.float32)
    hidden = pair * jax.nn.sigmoid(pair) * pltpu.roll(pair, HALF, 1)
    lane = lax.broadcasted_iota(jnp.int32, hidden.shape, 1)
    hidden_ref[:, 5 * LANES :] = jnp.where(lane < HALF, hidden, 0.0).astype(jnp.bfloat16)

    def down_step(n):
        both = jnp.concatenate([down(k, n) for k in range(6)], axis=1)
        terms = nt_dot(hidden_ref[...], both).astype(jnp.bfloat16)
        out_mine_ref[:, lanes(n, WIDE)] = terms[:half]
        out_other_ref[:, lanes(n, WIDE)] = terms[half:]

    steps(8, down_step, looped[1])


def first_ffn_kernel(mine_ref, other_ref, *refs):
    a_refs, b_refs = refs[:8], refs[8:13]
    y = lax.axis_index("y")
    cut = b_refs[2].shape[1]

    def block_a(k, n):
        return jnp.concatenate([a_refs[n][lax.rem(y + q, 4), k] for q in range(4)], axis=0)

    def block_b(k, n):
        across = b_refs[2][n, k] if k < cut else b_refs[3][n, k - cut]
        return jnp.concatenate([b_refs[0][n, k], b_refs[1][n, k], across, b_refs[4][n, k]], axis=0)

    def tile(k):
        block, which = (block_a, 6 + k) if k < 2 else (block_b, k - 2)
        return jnp.concatenate([block(which, n) for n in range(8)], axis=0)

    ffn_steps((False, False), tile, block_a, mine_ref, other_ref, *refs[13:])


def ffn_kernel(mine_ref, other_ref, packed_ref, *refs):
    def down(k, n):
        return packed_ref[pl.ds(n * 4, 4), k].reshape(-1, LANES)

    ffn_steps(FFN_LOOPED, lambda k: packed_ref[:, 6 + k].reshape(-1, LANES), down, mine_ref, other_ref, *refs)


def ffn_terms(rows, kernel, weights):
    half, width = rows[0].shape
    scratch = [
        pltpu.VMEM((2 * half, 6 * LANES), jnp.bfloat16),
        pltpu.VMEM((2 * half, width), jnp.bfloat16),
    ]
    outs = [pltpu.VMEM((half, width), jnp.bfloat16)] * 2
    return vmem_call(kernel, outs, scratch)(*rows, *weights)


def shifted(values, by, fill):
    row = lax.broadcasted_iota(jnp.int32, values.shape, 0)
    return jnp.where(row >= by, pltpu.roll(values, by, 0), fill)


def minus_expm1(x):
    series = 1.0 + x / 8.0
    for k in range(7, 1, -1):
        series = 1.0 + (x / k) * series
    return jnp.where(x > -0.5, -x * series, 1.0 - jnp.exp(x))


def scanned(keep, drive):
    by = 1
    while by < keep.shape[0]:
        drive = keep * shifted(drive, by, 0.0) + drive
        keep = keep * shifted(keep, by, 1.0)
        by *= 2
    return drive


def mixer_kernel(
    mine_ref, other_ref, packed_ref, taps_ref, a_ref, b_ref, rate_ref, out_mine_ref, out_other_ref, order_ref
):
    half = mine_ref.shape[0]
    chips = lax.axis_size("x")
    block = half // chips
    core = lax.axis_index("c")


    def tile(k, n):
        return packed_ref[pl.ds(n * 4, 4), k].reshape(-1, LANES)

    weights = [jnp.concatenate([tile(k, n) for n in range(8)], axis=0) for k in range(3)]
    weights = jnp.concatenate(weights, axis=1)
    places = []
    for n, ref in enumerate((mine_ref, other_ref)):
        part = jnp.dot(ref[...], weights, preferred_element_type=jnp.float32)
        which = core if n == 0 else 1 - core
        for chip in range(chips):
            place = pl.multiple_of((chip * 2 + which) * block, block)
            places.append(place)
            order_ref[pl.ds(place, block), :] = part[chip * block : (chip + 1) * block]
    z = order_ref[:, : 2 * LANES]
    ends = order_ref[:, 2 * LANES :]
    lane = lax.broadcasted_iota(jnp.int32, ends.shape, 1)
    groups = (
        (z[:, :LANES], z[:, LANES:]),
        (jnp.where(lane < HALF, ends, 0.0), pltpu.roll(ends, HALF, 1)),
    )
    mixed = []
    for g, (lru_x, lru_gate) in enumerate(groups):
        lru_x = lru_x.astype(jnp.bfloat16).astype(jnp.float32)
        lru_gate = lru_gate.astype(jnp.bfloat16).astype(jnp.float32)
        own = slice(g * LANES, (g + 1) * LANES)
        taps = taps_ref[:, own]
        conv = taps[0:1] * lru_x
        for k in range(1, 4):
            conv = conv + taps[k : k + 1] * shifted(lru_x, k, 0.0)
        low = conv.astype(jnp.bfloat16)
        recall = jax.nn.sigmoid(jnp.dot(low, a_ref[g], preferred_element_type=jnp.float32))
        admit = jax.nn.sigmoid(jnp.dot(low, b_ref[g], preferred_element_type=jnp.float32))
        log_keep = recall * rate_ref[:, own]
        drive = jnp.sqrt(minus_expm1(2.0 * log_keep)) * admit * low.astype(jnp.float32)
        state = scanned(jnp.exp(log_keep), drive)
        mixed.append(state * jax.nn.gelu(lru_gate))
    for g in range(2):
        order_ref[:, g * LANES : (g + 1) * LANES] = mixed[g]
    mixed = jnp.concatenate([order_ref[pl.ds(p, block), : 2 * LANES] for p in places], axis=0)
    mixed = mixed.astype(jnp.bfloat16)
    full = mixed[:, :LANES]
    short = mixed[:, LANES : LANES + HALF]

    def out_step(n):
        terms = nt_dot(full, tile(3, n)) + nt_dot(short, tile(4, n)[:, :HALF])
        terms = terms.astype(jnp.bfloat16)
        out_mine_ref[:, lanes(n, WIDE)] = terms[:half]
        out_other_ref[:, lanes(n, WIDE)] = terms[half:]

    steps(8, out_step, True)


def paired_blocks(blocks):
    zero = jnp.zeros_like(blocks[0])
    top = jnp.concatenate(
        [jnp.concatenate([blocks[0], zero], 1), jnp.concatenate([zero, blocks[1]], 1)], 0
    )
    end = jnp.concatenate(
        [jnp.concatenate([blocks[2], zero], 1), jnp.concatenate([zero, zero], 1)], 0
    )
    return jnp.stack([top, end])


def mixer_terms(rows, packed, conv_weight, gate_a_weight, gate_x_weight, decay_param):
    half, width = rows[0].shape
    pad = ((0, 0), (0, HALF))
    taps = jnp.pad(conv_weight.astype(jnp.float32), pad)
    rate = jnp.pad(-8.0 * jax.nn.softplus(-decay_param)[None], pad)
    outs = [pltpu.VMEM((half, width), jnp.bfloat16)] * 2
    scratch = [pltpu.VMEM((2 * half, 3 * LANES), jnp.float32)]
    return vmem_call(mixer_kernel, outs, scratch)(
        *rows, packed, taps, paired_blocks(gate_a_weight), paired_blocks(gate_x_weight), rate
    )


def body(
    tokens,
    ffn1_gain,
    ffn1_gate,
    ffn1_up,
    ffn1_down,
    mix_gain,
    lru_in_weight,
    lru_gate_weight,
    conv_weight,
    gate_a_weight,
    gate_x_weight,
    decay_param,
    mix_out_weight,
    ffn2_gain,
    ffn2_gate,
    ffn2_up,
    ffn2_down,
):
    ends = [((1, 640, HALF), (2, 640, HALF))]
    gates, uppers = full_tiles(1, 5), full_tiles(2, 5)
    downs = full_tiles(0, 5) + [((0, 640, HALF),)]
    order = gates + uppers + ends
    mixing = full_tiles(3, 1) + full_tiles(4, 1) + [((3, LANES, HALF), (4, LANES, HALF))]
    mixing += full_tiles(5, 1) + [((5, LANES, HALF),)]
    from_two = [tuple((which + 6, at, size) for which, at, size in p) for p in downs + order]
    own, others, mixing, second = packed_tiles(
        downs + order + mixing + from_two,
        [
            *(ffn1_down.T, ffn1_gate, ffn1_up),
            *(lru_in_weight, lru_gate_weight, mix_out_weight.T),
            *(ffn2_down.T, ffn2_gate, ffn2_up),
        ],
        (8, 9, 5, 17),
        (1, 1, 1, 1),
    )
    packed_mixing = gather_tiles(mixing)
    packed = gather_tiles(second)
    own = lax.all_gather(own, "y", axis=0)
    block, *far = spread_over_z(others)
    weights = spread_z_last(own, *far) + spread_over_y(block)

    normed = turned_norm(tokens, ffn1_gain)
    normed = after(normed, block)
    rows = gather_rows(normed)
    sums = sent_sums(ffn_terms(rows, first_ffn_kernel, weights))
    first, normed = combined(tokens, sums, True, "zy", mix_gain)
    (packed_mixing,) = in_vmem(packed_mixing)
    normed, packed_mixing = lax.optimization_barrier((normed, packed_mixing))
    rows = gather_rows(normed)
    sums = sent_sums(
        mixer_terms(rows, packed_mixing, conv_weight, gate_a_weight, gate_x_weight, decay_param),
    )
    second, normed = combined(first, sums, False, "", ffn2_gain)
    rows = gather_rows(normed)
    sums = last_sums(ffn_terms(rows, ffn_kernel, [packed]))
    return combined(second, sums, True)[0]


def solution(mesh):
    split = Mesh(mesh.devices.reshape(8, 4, 4, 2), FS_TP)
    placed = (
        P(FS_TP, None),
        P(),
        P(FS, TP),
        P(FS, TP),
        P(TP, FS),
        P(),
        P(FS, TP),
        P(FS, TP),
        P(None, TP),
        P(TP, None, None),
        P(TP, None, None),
        P(TP),
        P(TP, FS),
        P(),
        P(FS, TP),
        P(FS, TP),
        P(TP, FS),
    )

    return jax.shard_map(
        body, mesh=split, in_specs=placed, out_specs=P(FS_TP, None), check_vma=False
    )
```

```python
import jax
import jax.numpy as jnp
from jax import lax
from jax.experimental import pallas as pl
from jax.experimental.pallas import tpu as pltpu
from jax.sharding import Mesh
from jax.sharding import PartitionSpec as P

FS = ("z", "y")
TP = ("x", "c")
FS_TP = ("z", "y", "x", "c")

EPS = 1e-06
LANES = 128
SHARD = 64
HALF = 64
WIDE = 256
PARAMS = pltpu.CompilerParams(vmem_limit_bytes=24 << 20)


def moved(value, axis, by):
    count = lax.axis_size(axis)
    return lax.ppermute(value, axis, [(i, (i - by) % count) for i in range(count)])


def in_vmem(*values):
    return tuple(pltpu.with_memory_space_constraint(v, pltpu.VMEM) for v in values)


def vmem_specs(count):
    return [pl.BlockSpec(memory_space=pltpu.VMEM)] * count


def vmem_call(kernel, out_shape, scratch=()):
    def call(*args):
        return pl.pallas_call(
            kernel,
            in_specs=vmem_specs(len(args)),
            out_specs=jax.tree.map(lambda _: vmem_specs(1)[0], out_shape),
            out_shape=out_shape,
            scratch_shapes=list(scratch),
            compiler_params=PARAMS,
        )(*in_vmem(*args))

    return call


def norm_of(wide, gain):
    scale = lax.rsqrt(jnp.mean(wide * wide, axis=-1, keepdims=True) + EPS)
    return (wide * scale * gain).astype(jnp.bfloat16)


def turned_by_y(values, amount):
    groups = range(0, values.shape[1], WIDE)
    return jnp.concatenate([pltpu.roll(values[:, g : g + WIDE], amount, 1) for g in groups], axis=1)


def turned_to(values, axes):
    z, y = lax.axis_index("z"), lax.axis_index("y")
    if "z" in axes:
        values = pltpu.roll(values, lax.rem(8 - z, 8) * WIDE, 1)
    if "y" in axes:
        values = turned_by_y(values, lax.rem(4 - y, 4) * SHARD)
    return values


def turned_back(values, axes):
    z, y = lax.axis_index("z"), lax.axis_index("y")
    if "y" in axes:
        values = turned_by_y(values, y * SHARD)
    if "z" in axes:
        values = pltpu.roll(values, z * WIDE, 1)
    return values


def turned_norm_of(wide, gain, axes):
    normed = norm_of(wide, gain)
    if axes:
        normed = turned_to(normed.astype(jnp.float32), axes).astype(jnp.bfloat16)
    return normed


def norm_kernel(rows_ref, gain_ref, out_ref):
    out_ref[...] = turned_norm_of(rows_ref[...].astype(jnp.float32), gain_ref[...], "zy")


def turned_norm(values, gain):
    out = pltpu.VMEM(values.shape, jnp.bfloat16)
    return vmem_call(norm_kernel, out)(values, gain[None])


def gather_rows(own):
    mine = lax.all_gather(own, "x", axis=0, tiled=True)
    return mine, moved(mine, "c", 1)


def pair_sum_kernel(mine_ref, other_ref, out_ref):
    rows = out_ref.shape[1]
    for n in range(out_ref.shape[0]):
        own = slice(n * rows, (n + 1) * rows)
        out_ref[n] = (
            mine_ref[own].astype(jnp.float32) + other_ref[own].astype(jnp.float32)
        ).astype(jnp.bfloat16)


def sent_sums(terms):
    mine, other = terms
    count = lax.axis_size("x")
    out = pltpu.VMEM((count, mine.shape[0] // count, mine.shape[1]), jnp.bfloat16)
    other = moved(other, "c", 1)
    sums = vmem_call(pair_sum_kernel, out)(mine, other)
    return [lax.all_to_all(sums, "x", split_axis=0, concat_axis=0, tiled=True)]


def apart_kernel(mine_ref, other_ref, *out_refs):
    rows, chips = out_refs[0].shape[0], len(out_refs)
    for n, out_ref in enumerate(out_refs):
        chip = lax.rem(lax.axis_index("x") + n, chips)
        own = pl.ds(pl.multiple_of(chip * rows, rows), rows)
        out_ref[...] = (
            mine_ref[own].astype(jnp.float32) + other_ref[own].astype(jnp.float32)
        ).astype(jnp.bfloat16)


def last_sums(terms):
    mine, other = terms
    count = lax.axis_size("x")
    outs = [pltpu.VMEM((mine.shape[0] // count, mine.shape[1]), jnp.bfloat16)] * count
    sums = vmem_call(apart_kernel, outs)(mine, moved(other, "c", 1))
    return [sums[0]] + [moved(sums[n], "x", -n) for n in range(1, count)]


def combine_kernel(half, turned, turn, parts, base_ref, *refs):
    sums, refs = refs[:parts], refs[parts:]
    if parts == 1:
        sums = [sums[0].at[n] for n in range(sums[0].shape[0])]
    total = sums[0][...].astype(jnp.float32)
    for part_ref in sums[1:]:
        total = total + part_ref[...].astype(jnp.float32)
    total = turned_back(total, turned)
    if half:
        total = 0.5 * total
    result = (base_ref[...].astype(jnp.float32) + total).astype(jnp.bfloat16)
    if len(refs) == 1:
        refs[0][...] = result
    else:
        gain_ref, out_ref, norm_ref = refs
        out_ref[...] = result
        norm_ref[...] = turned_norm_of(result.astype(jnp.float32), gain_ref[...], turn)


def combined(base, sums, half, turned="", gain=None, turn=""):
    shape = pltpu.VMEM(base.shape, jnp.bfloat16)
    extra = () if gain is None else (gain[None],)
    outs = [shape] * 2 if extra else [jax.ShapeDtypeStruct(base.shape, jnp.bfloat16)]
    kernel = lambda *refs: combine_kernel(half, turned, turn, len(sums), *refs)
    return vmem_call(kernel, outs)(base, *sums, *extra)


def pack_kernel(plan, out_copies, counts, *refs):
    in_refs, out_refs = refs[: -len(counts)], refs[-len(counts) :]
    places = [
        (ref, k, copies)
        for ref, count, copies in zip(out_refs, counts, out_copies)
        for k in range(count)
    ]
    for (out_ref, n, copies), parts in zip(places, plan):
        pieces = [in_refs[which][:, at : at + size] for which, at, size in parts]
        if len(pieces) == 2:
            low, high = (p.astype(jnp.float32) for p in pieces)
            tile = jnp.concatenate([low, high], axis=1).astype(jnp.bfloat16)
        else:
            tile = pieces[0]
        size = tile.shape[1]
        for at in [()] if copies == 1 else [(k,) for k in range(copies)]:
            if size < LANES:
                out_ref[(*at, n)] = jnp.zeros((SHARD, LANES), jnp.bfloat16)
            out_ref[(*at, n, slice(None), slice(0, size))] = tile


def packed_tiles(plan, arrays, counts, out_copies):
    shapes = [
        jax.ShapeDtypeStruct((*((k,) if k > 1 else ()), n, SHARD, LANES), jnp.bfloat16)
        for n, k in zip(counts, out_copies)
    ]
    return pl.pallas_call(
        lambda *refs: pack_kernel(plan, out_copies, counts, *refs),
        out_shape=shapes,
        compiler_params=PARAMS,
        name="pack",
    )(*[in_hbm(a) for a in arrays])


def gather_tiles(packed):
    full = lax.all_gather(packed.reshape(-1, LANES), FS, axis=0, tiled=True)
    return full.reshape(-1, *packed.shape)


def fetch_kernel(in_ref, out_ref, sem):
    copy = pltpu.make_async_copy(in_ref, out_ref, sem)
    copy.start()
    copy.wait()


def fetched(value):
    return pl.pallas_call(
        fetch_kernel,
        in_specs=[pl.BlockSpec(memory_space=pl.ANY)],
        out_specs=vmem_specs(1)[0],
        out_shape=pltpu.VMEM(value.shape, value.dtype),
        scratch_shapes=[pltpu.SemaphoreType.DMA],
        compiler_params=PARAMS,
        name="copy_in",
    )(in_hbm(value))


def full_tiles(which, count):
    return [((which, k * LANES, LANES),) for k in range(count)]


def after(value, *others):
    return lax.optimization_barrier((value, *others))[0]


def in_hbm(value):
    return pltpu.with_memory_space_constraint(value, pltpu.HBM)


def both_ways(up, down, axis):
    return lax.optimization_barrier((moved(up, axis, 1), moved(down, axis, -1)))


def spread_z_last(block, *others):
    up = down = after(block, *others)
    ups, downs = [block], []
    for _ in range(1, 4):
        up, down = both_ways(up, down, "z")
        ups.append(up)
        downs.insert(0, down)
    return [*ups, moved(up, "z", 1), *downs]


def join_kernel(*refs):
    *part_refs, out_ref = refs
    for n, ref in enumerate(part_refs):
        out_ref[n] = ref[...]


def spread_over_z(own):
    up = down = own
    ups, downs = [own], []
    for _ in range(1, 4):
        up, down = both_ways(up, down, "z")
        ups.append(up)
        downs.insert(0, down)
    parts = [*ups, moved(up, "z", 1), *downs]
    out = pltpu.VMEM((8, *own.shape), jnp.bfloat16)
    return vmem_call(join_kernel, out)(*parts), up, down


def spread_over_y(block):
    up, down = both_ways(block, block, "y")
    cut = (block.shape[1] + 1) // 2
    across = [moved(up[:, :cut], "y", 1), moved(down[:, cut:], "y", -1)]
    return [block, up, *across, down]


def nt_dot(a, b):
    return lax.dot_general(a, b, (((1,), (1,)), ((), ())), preferred_element_type=jnp.float32)


def steps(count, step, looped):
    if looped:
        lax.fori_loop(0, count, lambda n, carry: (step(n), carry)[1], 0)
    else:
        for n in range(count):
            step(n)


def lanes(n, size):
    return pl.ds(n * size if isinstance(n, int) else pl.multiple_of(n * size, size), size)


def ffn_steps(tile, down, mine_ref, other_ref, out_mine_ref, out_other_ref, hidden_ref, rows_ref):
    half = mine_ref.shape[0]
    rows_ref[:half] = mine_ref[...]
    rows_ref[half:] = other_ref[...]

    def hidden_step(n):
        both = jnp.concatenate([tile(n), tile(5 + n)], axis=1)
        pair = jnp.dot(rows_ref[...], both, preferred_element_type=jnp.float32)
        hidden = pair[:, :LANES] * jax.nn.sigmoid(pair[:, :LANES]) * pair[:, LANES:]
        hidden_ref[:, lanes(n, LANES)] = hidden.astype(jnp.bfloat16)

    steps(5, hidden_step, False)
    pair = jnp.dot(rows_ref[...], tile(10), preferred_element_type=jnp.float32)
    hidden = pair * jax.nn.sigmoid(pair) * pltpu.roll(pair, HALF, 1)
    lane = lax.broadcasted_iota(jnp.int32, hidden.shape, 1)
    hidden_ref[:, 5 * LANES :] = jnp.where(lane < HALF, hidden, 0.0).astype(jnp.bfloat16)

    def down_step(n):
        both = jnp.concatenate([down(k, n) for k in range(6)], axis=1)
        terms = nt_dot(hidden_ref[...], both).astype(jnp.bfloat16)
        out_mine_ref[:, lanes(n, WIDE)] = terms[:half]
        out_other_ref[:, lanes(n, WIDE)] = terms[half:]

    steps(8, down_step, False)


def first_ffn_kernel(mine_ref, other_ref, *refs):
    a_refs, b_refs = refs[:8], refs[8:13]
    y = lax.axis_index("y")
    cut = b_refs[2].shape[1]

    def block_a(k, n):
        return jnp.concatenate([a_refs[n][lax.rem(y + q, 4), k] for q in range(4)], axis=0)

    def block_b(k, n):
        across = b_refs[2][n, k] if k < cut else b_refs[3][n, k - cut]
        return jnp.concatenate([b_refs[0][n, k], b_refs[1][n, k], across, b_refs[4][n, k]], axis=0)

    def tile(k):
        block, which = (block_a, 6 + k) if k < 2 else (block_b, k - 2)
        return jnp.concatenate([block(which, n) for n in range(8)], axis=0)

    ffn_steps(tile, block_a, mine_ref, other_ref, *refs[13:])


def ffn_kernel(
    mine_ref, other_ref, packed_ref, out_mine_ref, out_other_ref, hidden_ref, rows_ref, store_ref, sum_ref, sems
):
    half = mine_ref.shape[0]
    tiles = store_ref.shape[1]

    def copy(n):
        own = pl.ds(n * 4, 4)
        return pltpu.make_async_copy(packed_ref.at[own], store_ref.at[own], sems.at[n])

    for n in range(8):
        copy(n).start()
    rows_ref[:half] = mine_ref[...]
    rows_ref[half:] = other_ref[...]
    sum_ref[...] = jnp.zeros_like(sum_ref)

    def chunk(n, carry):
        copy(n).wait()
        own = pl.ds(n * 4, 4)
        both = jnp.concatenate([store_ref[own, k].reshape(-1, LANES) for k in range(6, tiles)], axis=1)
        part = rows_ref[:, lanes(n, WIDE)]
        sum_ref[...] += jnp.dot(part, both, preferred_element_type=jnp.float32)
        return carry

    lax.fori_loop(0, 8, chunk, 0)
    for n in range(5):
        gate = sum_ref[:, lanes(n, LANES)]
        hidden = gate * jax.nn.sigmoid(gate) * sum_ref[:, lanes(5 + n, LANES)]
        hidden_ref[:, lanes(n, LANES)] = hidden.astype(jnp.bfloat16)
    pair = sum_ref[:, lanes(10, LANES)]
    hidden = pair * jax.nn.sigmoid(pair) * pltpu.roll(pair, HALF, 1)
    lane = lax.broadcasted_iota(jnp.int32, hidden.shape, 1)
    hidden_ref[:, lanes(5, LANES)] = jnp.where(lane < HALF, hidden, 0.0).astype(jnp.bfloat16)
    for n in range(8):
        own = pl.ds(n * 4, 4)
        both = jnp.concatenate([store_ref[own, k].reshape(-1, LANES) for k in range(6)], axis=1)
        terms = nt_dot(hidden_ref[...], both).astype(jnp.bfloat16)
        out_mine_ref[:, lanes(n, WIDE)] = terms[:half]
        out_other_ref[:, lanes(n, WIDE)] = terms[half:]


def ffn_scratch(half, width):
    return [
        pltpu.VMEM((2 * half, 6 * LANES), jnp.bfloat16),
        pltpu.VMEM((2 * half, width), jnp.bfloat16),
    ]


def first_ffn_terms(rows, weights):
    outs = [pltpu.VMEM(rows[0].shape, jnp.bfloat16)] * 2
    call = vmem_call(first_ffn_kernel, outs, ffn_scratch(*rows[0].shape))
    return call(*rows, *weights)


def ffn_terms(rows, packed):
    half, width = rows[0].shape
    return pl.pallas_call(
        ffn_kernel,
        in_specs=vmem_specs(2) + [pl.BlockSpec(memory_space=pl.ANY)],
        out_specs=vmem_specs(2),
        out_shape=[pltpu.VMEM((half, width), jnp.bfloat16)] * 2,
        scratch_shapes=[
            *ffn_scratch(half, width),
            pltpu.VMEM(packed.shape, jnp.bfloat16),
            pltpu.VMEM((2 * half, (packed.shape[1] - 6) * LANES), jnp.float32),
            pltpu.SemaphoreType.DMA((8,)),
        ],
        compiler_params=PARAMS,
        name="ffn",
    )(*in_vmem(*rows), in_hbm(packed))


def shifted(values, by, fill):
    row = lax.broadcasted_iota(jnp.int32, values.shape, 0)
    return jnp.where(row >= by, pltpu.roll(values, by, 0), fill)


def minus_expm1(x):
    series = 1.0 + x / 8.0
    for k in range(7, 1, -1):
        series = 1.0 + (x / k) * series
    return jnp.where(x > -0.5, -x * series, 1.0 - jnp.exp(x))


def scanned(keep, drive):
    by = 1
    while by < keep.shape[0]:
        drive = keep * shifted(drive, by, 0.0) + drive
        keep = keep * shifted(keep, by, 1.0)
        by *= 2
    return drive


def mixer_kernel(
    mine_ref, other_ref, packed_ref, taps_ref, a_ref, b_ref, rate_ref, out_mine_ref, out_other_ref, order_ref
):
    half = mine_ref.shape[0]
    chips = lax.axis_size("x")
    block = half // chips
    core = lax.axis_index("c")


    def tile(k, n):
        return packed_ref[pl.ds(n * 4, 4), k].reshape(-1, LANES)

    weights = [jnp.concatenate([tile(k, n) for n in range(8)], axis=0) for k in range(3)]
    weights = jnp.concatenate(weights, axis=1)
    places = []
    for n, ref in enumerate((mine_ref, other_ref)):
        part = jnp.dot(ref[...], weights, preferred_element_type=jnp.float32)
        which = core if n == 0 else 1 - core
        for chip in range(chips):
            place = pl.multiple_of((chip * 2 + which) * block, block)
            places.append(place)
            order_ref[pl.ds(place, block), :] = part[chip * block : (chip + 1) * block]
    z = order_ref[:, : 2 * LANES]
    ends = order_ref[:, 2 * LANES :]
    lane = lax.broadcasted_iota(jnp.int32, ends.shape, 1)
    groups = (
        (z[:, :LANES], z[:, LANES:]),
        (jnp.where(lane < HALF, ends, 0.0), pltpu.roll(ends, HALF, 1)),
    )
    mixed = []
    for g, (lru_x, lru_gate) in enumerate(groups):
        lru_x = lru_x.astype(jnp.bfloat16).astype(jnp.float32)
        lru_gate = lru_gate.astype(jnp.bfloat16).astype(jnp.float32)
        own = slice(g * LANES, (g + 1) * LANES)
        taps = taps_ref[:, own]
        conv = taps[0:1] * lru_x
        for k in range(1, 4):
            conv = conv + taps[k : k + 1] * shifted(lru_x, k, 0.0)
        low = conv.astype(jnp.bfloat16)
        recall = jax.nn.sigmoid(jnp.dot(low, a_ref[g], preferred_element_type=jnp.float32))
        admit = jax.nn.sigmoid(jnp.dot(low, b_ref[g], preferred_element_type=jnp.float32))
        log_keep = recall * rate_ref[:, own]
        drive = jnp.sqrt(minus_expm1(2.0 * log_keep)) * admit * low.astype(jnp.float32)
        state = scanned(jnp.exp(log_keep), drive)
        mixed.append(state * jax.nn.gelu(lru_gate))
    for g in range(2):
        order_ref[:, g * LANES : (g + 1) * LANES] = mixed[g]
    mixed = jnp.concatenate([order_ref[pl.ds(p, block), : 2 * LANES] for p in places], axis=0)
    mixed = mixed.astype(jnp.bfloat16)
    full = mixed[:, :LANES]
    short = mixed[:, LANES : LANES + HALF]

    def out_step(n):
        terms = nt_dot(full, tile(3, n)) + nt_dot(short, tile(4, n)[:, :HALF])
        terms = terms.astype(jnp.bfloat16)
        out_mine_ref[:, lanes(n, WIDE)] = terms[:half]
        out_other_ref[:, lanes(n, WIDE)] = terms[half:]

    steps(8, out_step, True)


def paired_blocks(blocks):
    zero = jnp.zeros_like(blocks[0])
    top = jnp.concatenate(
        [jnp.concatenate([blocks[0], zero], 1), jnp.concatenate([zero, blocks[1]], 1)], 0
    )
    end = jnp.concatenate(
        [jnp.concatenate([blocks[2], zero], 1), jnp.concatenate([zero, zero], 1)], 0
    )
    return jnp.stack([top, end])


def mixer_terms(rows, packed, conv_weight, gate_a_weight, gate_x_weight, decay_param):
    half, width = rows[0].shape
    pad = ((0, 0), (0, HALF))
    taps = jnp.pad(conv_weight.astype(jnp.float32), pad)
    rate = jnp.pad(-8.0 * jax.nn.softplus(-decay_param)[None], pad)
    outs = [pltpu.VMEM((half, width), jnp.bfloat16)] * 2
    scratch = [pltpu.VMEM((2 * half, 3 * LANES), jnp.float32)]
    return vmem_call(mixer_kernel, outs, scratch)(
        *rows, packed, taps, paired_blocks(gate_a_weight), paired_blocks(gate_x_weight), rate
    )


def body(
    tokens,
    ffn1_gain,
    ffn1_gate,
    ffn1_up,
    ffn1_down,
    mix_gain,
    lru_in_weight,
    lru_gate_weight,
    conv_weight,
    gate_a_weight,
    gate_x_weight,
    decay_param,
    mix_out_weight,
    ffn2_gain,
    ffn2_gate,
    ffn2_up,
    ffn2_down,
):
    ends = [((1, 640, HALF), (2, 640, HALF))]
    gates, uppers = full_tiles(1, 5), full_tiles(2, 5)
    downs = full_tiles(0, 5) + [((0, 640, HALF),)]
    order = gates + uppers + ends
    mixing = full_tiles(3, 1) + full_tiles(4, 1) + [((3, LANES, HALF), (4, LANES, HALF))]
    mixing += full_tiles(5, 1) + [((5, LANES, HALF),)]
    from_two = [tuple((which + 6, at, size) for which, at, size in p) for p in downs + order]
    own, others, mixing, second = packed_tiles(
        downs + order + mixing + from_two,
        [
            *(ffn1_down.T, ffn1_gate, ffn1_up),
            *(lru_in_weight, lru_gate_weight, mix_out_weight.T),
            *(ffn2_down.T, ffn2_gate, ffn2_up),
        ],
        (8, 9, 5, 17),
        (1, 1, 1, 1),
    )
    packed_mixing = gather_tiles(mixing)
    packed = gather_tiles(second)
    own = lax.all_gather(own, "y", axis=0)
    block, *far = spread_over_z(others)
    weights = spread_z_last(own, *far) + spread_over_y(block)

    normed = turned_norm(tokens, ffn1_gain)
    normed = after(normed, block)
    rows = gather_rows(normed)
    sums = sent_sums(first_ffn_terms(rows, weights))
    first, normed = combined(tokens, sums, True, "zy", mix_gain)
    packed_mixing = fetched(packed_mixing)
    rows = gather_rows(normed)
    sums = sent_sums(
        mixer_terms(rows, packed_mixing, conv_weight, gate_a_weight, gate_x_weight, decay_param),
    )
    second, normed = combined(first, sums, False, "", ffn2_gain)
    rows = gather_rows(normed)
    sums = last_sums(ffn_terms(rows, packed))
    return combined(second, sums, True)[0]


def solution(mesh):
    split = Mesh(mesh.devices.reshape(8, 4, 4, 2), FS_TP)
    placed = (
        P(FS_TP, None),
        P(),
        P(FS, TP),
        P(FS, TP),
        P(TP, FS),
        P(),
        P(FS, TP),
        P(FS, TP),
        P(None, TP),
        P(TP, None, None),
        P(TP, None, None),
        P(TP),
        P(TP, FS),
        P(),
        P(FS, TP),
        P(FS, TP),
        P(TP, FS),
    )

    return jax.shard_map(
        body, mesh=split, in_specs=placed, out_specs=P(FS_TP, None), check_vma=False
    )
```

```python
import jax
import jax.numpy as jnp
from jax import lax
from jax.experimental import pallas as pl
from jax.experimental.pallas import tpu as pltpu
from jax.sharding import Mesh
from jax.sharding import PartitionSpec as P

FS = ("z", "y")
TP = ("x", "c")
FS_TP = ("z", "y", "x", "c")

EPS = 1e-06
LANES = 128
SHARD = 64
HALF = 64
WIDE = 256
PARAMS = pltpu.CompilerParams(vmem_limit_bytes=24 << 20)


def moved(value, axis, by):
    count = lax.axis_size(axis)
    return lax.ppermute(value, axis, [(i, (i - by) % count) for i in range(count)])


def in_vmem(*values):
    return tuple(pltpu.with_memory_space_constraint(v, pltpu.VMEM) for v in values)


def vmem_specs(count):
    return [pl.BlockSpec(memory_space=pltpu.VMEM)] * count


def vmem_call(kernel, out_shape, scratch=()):
    def call(*args):
        return pl.pallas_call(
            kernel,
            in_specs=vmem_specs(len(args)),
            out_specs=jax.tree.map(lambda _: vmem_specs(1)[0], out_shape),
            out_shape=out_shape,
            scratch_shapes=list(scratch),
            compiler_params=PARAMS,
        )(*in_vmem(*args))

    return call


def norm_of(wide, gain):
    scale = lax.rsqrt(jnp.mean(wide * wide, axis=-1, keepdims=True) + EPS)
    return (wide * scale * gain).astype(jnp.bfloat16)


def turned_by_y(values, amount):
    groups = range(0, values.shape[1], WIDE)
    return jnp.concatenate([pltpu.roll(values[:, g : g + WIDE], amount, 1) for g in groups], axis=1)


def turned_to(values, axes):
    z, y = lax.axis_index("z"), lax.axis_index("y")
    if "z" in axes:
        values = pltpu.roll(values, lax.rem(8 - z, 8) * WIDE, 1)
    if "y" in axes:
        values = turned_by_y(values, lax.rem(4 - y, 4) * SHARD)
    return values


def turned_back(values, axes):
    z, y = lax.axis_index("z"), lax.axis_index("y")
    if "y" in axes:
        values = turned_by_y(values, y * SHARD)
    if "z" in axes:
        values = pltpu.roll(values, z * WIDE, 1)
    return values


def turned_norm_of(wide, gain, axes):
    normed = norm_of(wide, gain)
    if axes:
        normed = turned_to(normed.astype(jnp.float32), axes).astype(jnp.bfloat16)
    return normed


def norm_kernel(rows_ref, gain_ref, out_ref):
    out_ref[...] = turned_norm_of(rows_ref[...].astype(jnp.float32), gain_ref[...], "zy")


def turned_norm(values, gain):
    out = pltpu.VMEM(values.shape, jnp.bfloat16)
    return vmem_call(norm_kernel, out)(values, gain[None])


def gather_rows(own):
    mine = lax.all_gather(own, "x", axis=0, tiled=True)
    return mine, moved(mine, "c", 1)


def pair_sum_kernel(mine_ref, other_ref, out_ref):
    rows = out_ref.shape[1]
    for n in range(out_ref.shape[0]):
        own = slice(n * rows, (n + 1) * rows)
        out_ref[n] = (
            mine_ref[own].astype(jnp.float32) + other_ref[own].astype(jnp.float32)
        ).astype(jnp.bfloat16)


def sent_sums(terms):
    mine, other = terms
    count = lax.axis_size("x")
    out = pltpu.VMEM((count, mine.shape[0] // count, mine.shape[1]), jnp.bfloat16)
    other = moved(other, "c", 1)
    sums = vmem_call(pair_sum_kernel, out)(mine, other)
    return [lax.all_to_all(sums, "x", split_axis=0, concat_axis=0, tiled=True)]


def apart_kernel(mine_ref, other_ref, *out_refs):
    rows, chips = out_refs[0].shape[0], len(out_refs)
    for n, out_ref in enumerate(out_refs):
        chip = lax.rem(lax.axis_index("x") + n, chips)
        own = pl.ds(pl.multiple_of(chip * rows, rows), rows)
        out_ref[...] = (
            mine_ref[own].astype(jnp.float32) + other_ref[own].astype(jnp.float32)
        ).astype(jnp.bfloat16)


def last_sums(terms):
    mine, other = terms
    count = lax.axis_size("x")
    outs = [pltpu.VMEM((mine.shape[0] // count, mine.shape[1]), jnp.bfloat16)] * count
    sums = vmem_call(apart_kernel, outs)(mine, moved(other, "c", 1))
    return [sums[0]] + [moved(sums[n], "x", -n) for n in range(1, count)]


def combine_kernel(half, turned, turn, parts, base_ref, *refs):
    sums, refs = refs[:parts], refs[parts:]
    if parts == 1:
        sums = [sums[0].at[n] for n in range(sums[0].shape[0])]
    total = sums[0][...].astype(jnp.float32)
    for part_ref in sums[1:]:
        total = total + part_ref[...].astype(jnp.float32)
    total = turned_back(total, turned)
    if half:
        total = 0.5 * total
    result = (base_ref[...].astype(jnp.float32) + total).astype(jnp.bfloat16)
    if len(refs) == 1:
        refs[0][...] = result
    else:
        gain_ref, out_ref, norm_ref = refs
        out_ref[...] = result
        norm_ref[...] = turned_norm_of(result.astype(jnp.float32), gain_ref[...], turn)


def combined(base, sums, half, turned="", gain=None, turn=""):
    shape = pltpu.VMEM(base.shape, jnp.bfloat16)
    extra = () if gain is None else (gain[None],)
    outs = [shape] * 2 if extra else [jax.ShapeDtypeStruct(base.shape, jnp.bfloat16)]
    kernel = lambda *refs: combine_kernel(half, turned, turn, len(sums), *refs)
    return vmem_call(kernel, outs)(base, *sums, *extra)


def pack_kernel(plan, out_copies, counts, *refs):
    in_refs, out_refs = refs[: -len(counts)], refs[-len(counts) :]
    places = [
        (ref, k, copies)
        for ref, count, copies in zip(out_refs, counts, out_copies)
        for k in range(count)
    ]
    for (out_ref, n, copies), parts in zip(places, plan):
        pieces = [in_refs[which][:, at : at + size] for which, at, size in parts]
        if len(pieces) == 2:
            low, high = (p.astype(jnp.float32) for p in pieces)
            tile = jnp.concatenate([low, high], axis=1).astype(jnp.bfloat16)
        else:
            tile = pieces[0]
        size = tile.shape[1]
        for at in [()] if copies == 1 else [(k,) for k in range(copies)]:
            if size < LANES:
                out_ref[(*at, n)] = jnp.zeros((SHARD, LANES), jnp.bfloat16)
            out_ref[(*at, n, slice(None), slice(0, size))] = tile


def packed_tiles(plan, arrays, counts, out_copies):
    shapes = [
        jax.ShapeDtypeStruct((*((k,) if k > 1 else ()), n, SHARD, LANES), jnp.bfloat16)
        for n, k in zip(counts, out_copies)
    ]
    return pl.pallas_call(
        lambda *refs: pack_kernel(plan, out_copies, counts, *refs),
        out_shape=shapes,
        compiler_params=PARAMS,
        name="pack",
    )(*[in_hbm(a) for a in arrays])


def gather_tiles(packed):
    full = lax.all_gather(packed.reshape(-1, LANES), FS, axis=0, tiled=True)
    return full.reshape(-1, *packed.shape)


def fetch_kernel(in_ref, out_ref, sem):
    copy = pltpu.make_async_copy(in_ref, out_ref, sem)
    copy.start()
    copy.wait()


def fetched(value):
    return pl.pallas_call(
        fetch_kernel,
        in_specs=[pl.BlockSpec(memory_space=pl.ANY)],
        out_specs=vmem_specs(1)[0],
        out_shape=pltpu.VMEM(value.shape, value.dtype),
        scratch_shapes=[pltpu.SemaphoreType.DMA],
        compiler_params=PARAMS,
        name="copy_in",
    )(in_hbm(value))


def full_tiles(which, count):
    return [((which, k * LANES, LANES),) for k in range(count)]


def after(value, *others):
    return lax.optimization_barrier((value, *others))[0]


def in_hbm(value):
    return pltpu.with_memory_space_constraint(value, pltpu.HBM)


def both_ways(up, down, axis):
    return lax.optimization_barrier((moved(up, axis, 1), moved(down, axis, -1)))


def spread_z_last(block, *others):
    up = down = after(block, *others)
    ups, downs = [block], []
    for _ in range(1, 4):
        up, down = both_ways(up, down, "z")
        ups.append(up)
        downs.insert(0, down)
    return [*ups, moved(up, "z", 1), *downs]


def join_kernel(*refs):
    *part_refs, out_ref = refs
    for n, ref in enumerate(part_refs):
        out_ref[n] = ref[...]


def spread_over_z(own):
    up = down = own
    ups, downs = [own], []
    for _ in range(1, 4):
        up, down = both_ways(up, down, "z")
        ups.append(up)
        downs.insert(0, down)
    parts = [*ups, moved(up, "z", 1), *downs]
    out = pltpu.VMEM((8, *own.shape), jnp.bfloat16)
    return vmem_call(join_kernel, out)(*parts), up, down


def spread_over_y(block):
    up, down = both_ways(block, block, "y")
    cut = (block.shape[1] + 1) // 2
    across = [moved(up[:, :cut], "y", 1), moved(down[:, cut:], "y", -1)]
    return [block, up, *across, down]


def nt_dot(a, b):
    return lax.dot_general(a, b, (((1,), (1,)), ((), ())), preferred_element_type=jnp.float32)


def steps(count, step, looped):
    if looped:
        lax.fori_loop(0, count, lambda n, carry: (step(n), carry)[1], 0)
    else:
        for n in range(count):
            step(n)


def lanes(n, size):
    return pl.ds(n * size if isinstance(n, int) else pl.multiple_of(n * size, size), size)


def ffn_steps(tile, down, mine_ref, other_ref, out_mine_ref, out_other_ref, hidden_ref, rows_ref):
    half = mine_ref.shape[0]
    rows_ref[:half] = mine_ref[...]
    rows_ref[half:] = other_ref[...]

    def hidden_step(n):
        both = jnp.concatenate([tile(n), tile(5 + n)], axis=1)
        pair = jnp.dot(rows_ref[...], both, preferred_element_type=jnp.float32)
        hidden = pair[:, :LANES] * jax.nn.sigmoid(pair[:, :LANES]) * pair[:, LANES:]
        hidden_ref[:, lanes(n, LANES)] = hidden.astype(jnp.bfloat16)

    steps(5, hidden_step, False)
    pair = jnp.dot(rows_ref[...], tile(10), preferred_element_type=jnp.float32)
    hidden = pair * jax.nn.sigmoid(pair) * pltpu.roll(pair, HALF, 1)
    lane = lax.broadcasted_iota(jnp.int32, hidden.shape, 1)
    hidden_ref[:, 5 * LANES :] = jnp.where(lane < HALF, hidden, 0.0).astype(jnp.bfloat16)

    def down_step(n):
        both = jnp.concatenate([down(k, n) for k in range(6)], axis=1)
        terms = nt_dot(hidden_ref[...], both).astype(jnp.bfloat16)
        out_mine_ref[:, lanes(n, WIDE)] = terms[:half]
        out_other_ref[:, lanes(n, WIDE)] = terms[half:]

    steps(8, down_step, False)


def first_ffn_kernel(mine_ref, other_ref, *refs):
    a_refs, b_refs = refs[:8], refs[8:13]
    y = lax.axis_index("y")
    cut = b_refs[2].shape[1]

    def block_a(k, n):
        return jnp.concatenate([a_refs[n][lax.rem(y + q, 4), k] for q in range(4)], axis=0)

    def block_b(k, n):
        across = b_refs[2][n, k] if k < cut else b_refs[3][n, k - cut]
        return jnp.concatenate([b_refs[0][n, k], b_refs[1][n, k], across, b_refs[4][n, k]], axis=0)

    def tile(k):
        block, which = (block_a, 6 + k) if k < 2 else (block_b, k - 2)
        return jnp.concatenate([block(which, n) for n in range(8)], axis=0)

    ffn_steps(tile, block_a, mine_ref, other_ref, *refs[13:])


def ffn_kernel(
    mine_ref,
    other_ref,
    mixing_ref,
    packed_ref,
    out_mine_ref,
    out_other_ref,
    hidden_ref,
    rows_ref,
    store_ref,
    sum_ref,
    sems,
):
    half = mine_ref.shape[0]
    tiles = store_ref.shape[1]

    def copy(n):
        own = pl.ds(n * 4, 4)
        return pltpu.make_async_copy(packed_ref.at[own], store_ref.at[own], sems.at[n])

    for n in range(8):
        copy(n).start()
    rows_ref[:half] = mine_ref[...]
    rows_ref[half:] = other_ref[...]
    sum_ref[...] = jnp.zeros_like(sum_ref)

    def chunk(n, carry):
        copy(n).wait()
        own = pl.ds(n * 4, 4)
        both = jnp.concatenate([store_ref[own, k].reshape(-1, LANES) for k in range(5, tiles)], axis=1)
        part = rows_ref[:, lanes(n, WIDE)]
        sum_ref[...] += jnp.dot(part, both, preferred_element_type=jnp.float32)
        return carry

    lax.fori_loop(0, 8, chunk, 0)
    for n in range(5):
        gate = sum_ref[:, lanes(n, LANES)]
        hidden = gate * jax.nn.sigmoid(gate) * sum_ref[:, lanes(5 + n, LANES)]
        hidden_ref[:, lanes(n, LANES)] = hidden.astype(jnp.bfloat16)
    pair = sum_ref[:, lanes(10, LANES)]
    hidden = pltpu.roll(pair * jax.nn.sigmoid(pair), HALF, 1) * pair
    lane = lax.broadcasted_iota(jnp.int32, hidden.shape, 1)
    hidden_ref[:, lanes(5, LANES)] = jnp.where(lane >= HALF, hidden, 0.0).astype(jnp.bfloat16)
    for n in range(8):
        own = pl.ds(n * 4, 4)
        down = [store_ref[own, k] for k in range(5)] + [mixing_ref[own, 4]]
        both = jnp.concatenate([tile.reshape(-1, LANES) for tile in down], axis=1)
        terms = nt_dot(hidden_ref[...], both).astype(jnp.bfloat16)
        out_mine_ref[:, lanes(n, WIDE)] = terms[:half]
        out_other_ref[:, lanes(n, WIDE)] = terms[half:]


def ffn_scratch(half, width):
    return [
        pltpu.VMEM((2 * half, 6 * LANES), jnp.bfloat16),
        pltpu.VMEM((2 * half, width), jnp.bfloat16),
    ]


def first_ffn_terms(rows, weights):
    outs = [pltpu.VMEM(rows[0].shape, jnp.bfloat16)] * 2
    call = vmem_call(first_ffn_kernel, outs, ffn_scratch(*rows[0].shape))
    return call(*rows, *weights)


def ffn_terms(rows, mixing, packed):
    half, width = rows[0].shape
    return pl.pallas_call(
        ffn_kernel,
        in_specs=vmem_specs(3) + [pl.BlockSpec(memory_space=pl.ANY)],
        out_specs=vmem_specs(2),
        out_shape=[pltpu.VMEM((half, width), jnp.bfloat16)] * 2,
        scratch_shapes=[
            *ffn_scratch(half, width),
            pltpu.VMEM(packed.shape, jnp.bfloat16),
            pltpu.VMEM((2 * half, (packed.shape[1] - 5) * LANES), jnp.float32),
            pltpu.SemaphoreType.DMA((8,)),
        ],
        compiler_params=PARAMS,
        name="ffn",
    )(*in_vmem(*rows, mixing), in_hbm(packed))


def shifted(values, by, fill):
    row = lax.broadcasted_iota(jnp.int32, values.shape, 0)
    return jnp.where(row >= by, pltpu.roll(values, by, 0), fill)


def minus_expm1(x):
    series = 1.0 + x / 8.0
    for k in range(7, 1, -1):
        series = 1.0 + (x / k) * series
    return jnp.where(x > -0.5, -x * series, 1.0 - jnp.exp(x))


def scanned(keep, drive):
    by = 1
    while by < keep.shape[0]:
        drive = keep * shifted(drive, by, 0.0) + drive
        keep = keep * shifted(keep, by, 1.0)
        by *= 2
    return drive


def mixer_kernel(
    mine_ref, other_ref, packed_ref, taps_ref, a_ref, b_ref, rate_ref, out_mine_ref, out_other_ref, order_ref, group_ref
):
    half = mine_ref.shape[0]
    chips = lax.axis_size("x")
    block = half // chips
    core = lax.axis_index("c")


    def tile(k, n):
        return packed_ref[pl.ds(n * 4, 4), k].reshape(-1, LANES)

    weights = [jnp.concatenate([tile(k, n) for n in range(8)], axis=0) for k in range(3)]
    weights = jnp.concatenate(weights, axis=1)
    places = []
    for n, ref in enumerate((mine_ref, other_ref)):
        part = jnp.dot(ref[...], weights, preferred_element_type=jnp.float32)
        which = core if n == 0 else 1 - core
        for chip in range(chips):
            place = pl.multiple_of((chip * 2 + which) * block, block)
            places.append(place)
            order_ref[pl.ds(place, block), :] = part[chip * block : (chip + 1) * block]
    ends = order_ref[:, 2 * LANES :]
    lane = lax.broadcasted_iota(jnp.int32, ends.shape, 1)
    group_ref[0] = order_ref[:, : 2 * LANES]
    group_ref[1, :, :LANES] = jnp.where(lane < HALF, ends, 0.0)
    group_ref[1, :, LANES:] = pltpu.roll(ends, HALF, 1)

    def group(g, carry):
        lru_x = group_ref[g, :, :LANES].astype(jnp.bfloat16).astype(jnp.float32)
        lru_gate = group_ref[g, :, LANES:].astype(jnp.bfloat16).astype(jnp.float32)
        own = lanes(g, LANES)
        taps = taps_ref[:, own]
        conv = taps[0:1] * lru_x
        for k in range(1, 4):
            conv = conv + taps[k : k + 1] * shifted(lru_x, k, 0.0)
        low = conv.astype(jnp.bfloat16)
        recall = jax.nn.sigmoid(jnp.dot(low, a_ref[g], preferred_element_type=jnp.float32))
        admit = jax.nn.sigmoid(jnp.dot(low, b_ref[g], preferred_element_type=jnp.float32))
        log_keep = recall * rate_ref[:, own]
        drive = jnp.sqrt(minus_expm1(2.0 * log_keep)) * admit * low.astype(jnp.float32)
        state = scanned(jnp.exp(log_keep), drive)
        order_ref[:, own] = state * jax.nn.gelu(lru_gate)
        return carry

    lax.fori_loop(0, 2, group, 0)
    mixed = jnp.concatenate([order_ref[pl.ds(p, block), : 2 * LANES] for p in places], axis=0)
    mixed = mixed.astype(jnp.bfloat16)
    full = mixed[:, :LANES]
    short = mixed[:, LANES : LANES + HALF]

    def out_step(n):
        terms = nt_dot(full, tile(3, n)) + nt_dot(short, tile(4, n)[:, :HALF])
        terms = terms.astype(jnp.bfloat16)
        out_mine_ref[:, lanes(n, WIDE)] = terms[:half]
        out_other_ref[:, lanes(n, WIDE)] = terms[half:]

    steps(8, out_step, True)


def paired_blocks(blocks):
    zero = jnp.zeros_like(blocks[0])
    top = jnp.concatenate(
        [jnp.concatenate([blocks[0], zero], 1), jnp.concatenate([zero, blocks[1]], 1)], 0
    )
    end = jnp.concatenate(
        [jnp.concatenate([blocks[2], zero], 1), jnp.concatenate([zero, zero], 1)], 0
    )
    return jnp.stack([top, end])


def mixer_terms(rows, packed, conv_weight, gate_a_weight, gate_x_weight, decay_param):
    half, width = rows[0].shape
    pad = ((0, 0), (0, HALF))
    taps = jnp.pad(conv_weight.astype(jnp.float32), pad)
    rate = jnp.pad(-8.0 * jax.nn.softplus(-decay_param)[None], pad)
    outs = [pltpu.VMEM((half, width), jnp.bfloat16)] * 2
    scratch = [
        pltpu.VMEM((2 * half, 3 * LANES), jnp.float32),
        pltpu.VMEM((2, 2 * half, 2 * LANES), jnp.float32),
    ]
    return vmem_call(mixer_kernel, outs, scratch)(
        *rows, packed, taps, paired_blocks(gate_a_weight), paired_blocks(gate_x_weight), rate
    )


def body(
    tokens,
    ffn1_gain,
    ffn1_gate,
    ffn1_up,
    ffn1_down,
    mix_gain,
    lru_in_weight,
    lru_gate_weight,
    conv_weight,
    gate_a_weight,
    gate_x_weight,
    decay_param,
    mix_out_weight,
    ffn2_gain,
    ffn2_gate,
    ffn2_up,
    ffn2_down,
):
    ends = [((1, 640, HALF), (2, 640, HALF))]
    gates, uppers = full_tiles(1, 5), full_tiles(2, 5)
    downs = full_tiles(0, 5) + [((0, 640, HALF),)]
    order = gates + uppers + ends
    mixing = full_tiles(3, 1) + full_tiles(4, 1) + [((3, LANES, HALF), (4, LANES, HALF))]
    mixing += full_tiles(5, 1) + [((5, LANES, HALF), (6, 640, HALF))]
    from_two = [tuple((which + 6, at, size) for which, at, size in p) for p in downs[:5] + order]
    own, others, mixing, second = packed_tiles(
        downs + order + mixing + from_two,
        [
            *(ffn1_down.T, ffn1_gate, ffn1_up),
            *(lru_in_weight, lru_gate_weight, mix_out_weight.T),
            *(ffn2_down.T, ffn2_gate, ffn2_up),
        ],
        (8, 9, 5, 16),
        (1, 1, 1, 1),
    )
    packed_mixing = gather_tiles(mixing)
    packed = gather_tiles(second)
    own = lax.all_gather(own, "y", axis=0)
    block, *far = spread_over_z(others)
    weights = spread_z_last(own, *far) + spread_over_y(block)

    normed = turned_norm(tokens, ffn1_gain)
    normed = after(normed, block)
    rows = gather_rows(normed)
    sums = sent_sums(first_ffn_terms(rows, weights))
    first, normed = combined(tokens, sums, True, "zy", mix_gain)
    packed_mixing = fetched(packed_mixing)
    rows = gather_rows(normed)
    terms = mixer_terms(
        rows, packed_mixing, conv_weight, gate_a_weight, gate_x_weight, decay_param
    )
    sums = last_sums(terms)
    second, normed = combined(first, sums, False, "", ffn2_gain)
    rows = gather_rows(normed)
    sums = last_sums(ffn_terms(rows, packed_mixing, packed))
    return combined(second, sums, True)[0]


def solution(mesh):
    split = Mesh(mesh.devices.reshape(8, 4, 4, 2), FS_TP)
    placed = (
        P(FS_TP, None),
        P(),
        P(FS, TP),
        P(FS, TP),
        P(TP, FS),
        P(),
        P(FS, TP),
        P(FS, TP),
        P(None, TP),
        P(TP, None, None),
        P(TP, None, None),
        P(TP),
        P(TP, FS),
        P(),
        P(FS, TP),
        P(FS, TP),
        P(TP, FS),
    )

    return jax.shard_map(
        body, mesh=split, in_specs=placed, out_specs=P(FS_TP, None), check_vma=False
    )
```
